32 devices in a mesh: ep: 8 (over z, y), tp: 4 (over x, core).
Axes of the slice: x: 2, y: 2, z: 4, core: 2. Of those that a mesh axis runs over, the one named last changes fastest.
Arguments:
- tokens: bfloat16 [384, 2048], P(('ep', 'tp')), may hold values from -6 to 6
- cache_latent: bfloat16 [384, 1024, 512], P(('ep', 'tp')), may hold values from -1700 to 1700
- cache_rope: bfloat16 [384, 64, 1024], P(('ep', 'tp')), may hold values from -6 to 6
- lengths: int32 [384], P(('ep', 'tp')), may hold values from 128 to 1023, as said below
- attn_gain: bfloat16 [2048], replicated, may hold values from 0.099609375 to 1.8984375
- latent_gain: bfloat16 [512], replicated, may hold values from 0.099609375 to 1.8984375
- post_attn_gain: bfloat16 [2048], replicated, may hold values from 0.099609375 to 1.8984375
- ffn_gain: bfloat16 [2048], replicated, may hold values from 0.099609375 to 1.8984375
- post_ffn_gain: bfloat16 [2048], replicated, may hold values from 0.099609375 to 1.8984375
- w_query: bfloat16 [2048, 2048], P(None, 'tp'), may hold values from -0.125 to 0.125
- w_query_rot: bfloat16 [2048, 1024], P(None, 'tp'), may hold values from -0.125 to 0.125
- w_latent: bfloat16 [2048, 512], P(None, 'tp'), may hold values from -0.125 to 0.125
- w_key_rot: bfloat16 [2048, 64], replicated, may hold values from -0.125 to 0.125
- w_key_up: bfloat16 [512, 16, 128], P(None, 'tp'), may hold values from -0.25 to 0.25
- w_value_up: bfloat16 [512, 16, 128], P(None, 'tp'), may hold values from -0.25 to 0.25
- w_out: bfloat16 [2048, 2048], P('tp'), may hold values from -0.125 to 0.125
- route_logits: float32 [384, 4], P('ep'), may hold values from -6 to 6
- routes: int32 [384, 4], P('ep'), may hold values from 0 to 7, all different within a row; in each aligned block of 48 rows (0 to 47, 48 to 95, ...) at most 25 rows name the same one
- w_gate: bfloat16 [8, 2048, 2048], P('ep', None, 'tp'), may hold values from -0.3125 to 0.3125
- w_up: bfloat16 [8, 2048, 2048], P('ep', None, 'tp'), may hold values from -0.3125 to 0.3125
- w_down: bfloat16 [8, 2048, 2048], P('ep', 'tp'), may hold values from -0.125 to 0.125
Outputs:
- result: bfloat16 [384, 2048], P(('ep', 'tp'))
- new_latent: bfloat16 [384, 512], P(('ep', 'tp'))
- new_rope: bfloat16 [384, 64], P(('ep', 'tp'))
The draws below stay inside these ranges and needn't reach their ends.
Inputs may be any that keep to these rules, and one draw needn't show every extreme that they name: Each sequence's cache holds positions 0 to lengths - 1, and the new token stands at position lengths; some sequence has 1023 in every draw. `routes`: each row names 4 different experts; in each aligned block of 48 rows (the tokens of one index of ep) no expert is named more than 25 times, a bound that some block reaches.
All inputs are finite; a program needn't handle non-finite values.
Results may differ from the reference program's by a relative error of at most 0.019.
Values may be sent and summed in bfloat16 or wider, within the bound.
A program may use at most 128 MiB of HBM per device.

```python
import math
import jax
import jax.numpy as jnp
import numpy as np
from jax import lax

D = 2048
HEADS = 16
KEY_DIM = 128
ROT_DIM = 64
VAL_DIM = 128
LATENT = 512
FF = 2048
TOP_K = 4
SEQ_DEV = 12
LEN = 1024
EXPERTS = 8
GROUP = 48
BATCH = 384
CAP = 25
N_TP = 4


def draw_cache_latent(key, part):
    base_key = jax.random.fold_in(jax.random.fold_in(key, 11), 0)
    cache = jnp.clip(jax.random.normal(base_key, (BATCH, LEN, LATENT), jnp.float32), -5.0, 5.0)
    return cache.astype(jnp.bfloat16)


def draw_lengths(key, part):
    keys = jax.random.split(jax.random.fold_in(key, 23), 3)
    lowest = LEN // 8
    ceilings = jax.random.randint(keys[0], (BATCH // SEQ_DEV,), LEN // 4, LEN)
    ceilings = jnp.repeat(ceilings, SEQ_DEV)
    drawn = jax.random.randint(keys[1], (BATCH,), lowest, ceilings)
    longest = jax.random.randint(keys[2], (), 0, BATCH)
    return jnp.where(jnp.arange(BATCH) == longest, LEN - 1, drawn).astype(jnp.int32)


def block_levels(rng, shape, cuts, least, top_value):
    def one(position, shards_of):
        heights = jax.random.uniform(jax.random.fold_in(jax.random.fold_in(rng, 6), position), (shards_of,), jnp.float32, least / len(cuts), top_value / len(cuts))
        return jnp.repeat(jnp.exp(heights), shape[position] // shards_of).reshape((-1,) + (1,) * (len(shape) - position - 1))

    loudness = one(*cuts[0])
    for cut in cuts[1:]:
        loudness = loudness * one(*cut)
    return loudness


def assign_block(stream_key, own, number, rows, count, top, limit, lean):
    order = jax.random.permutation(stream_key, count)
    heavy_load, ordinary = shares(count, rows * top, limit, lean, True), shares(count, rows * top, limit, lean, False)
    places = jnp.arange(count)

    def named(sizes, offset_by):
        used = int((sizes > 0).sum())
        fixed = max(1, used // 4)
        shifted = fixed + (places - fixed + offset_by * (used - fixed)) % max(1, count - fixed)
        return jnp.zeros((count,), jnp.int32).at[order[jnp.where(places < fixed, places, shifted)]].set(jnp.asarray(sizes, jnp.int32))

    sizes = jnp.where(number % 4 == 0, named(heavy_load, number // 4), named(ordinary, number - number // 4 - 1))
    mixed = jax.random.permutation(jax.random.fold_in(own, 3), count)
    source_of, sink = mixed[0:count // 2 * 2:2], mixed[1:count // 2 * 2:2]
    room = jnp.minimum(sizes[source_of] - 1, limit - sizes[sink]) // 2
    room = jnp.where((source_of == order[0]) | (sink == order[0]) | (sizes[sink] == 0), 0, jnp.maximum(room, 0))
    shifted = jax.random.randint(jax.random.fold_in(own, 4), (count // 2,), 0, 1 << 20) % (room + 1)
    sizes = sizes.at[source_of].add(-shifted).at[sink].add(shifted)
    members = jnp.searchsorted(jnp.cumsum(sizes), jnp.arange(rows * top), side="right").astype(jnp.int32)
    table = members.reshape(top, rows).T
    table = table[jax.random.permutation(jax.random.fold_in(own, 1), rows)]
    offset_by = jax.random.randint(jax.random.fold_in(own, 2), (rows, 1), 0, top)
    return jnp.take_along_axis(table, (jnp.arange(top)[None, :] + offset_by) % top, axis=1)


def shares(number_of, total, bound, slope, full):
    loads = [(1 << 20) // math.isqrt(grade ** slope) + 1 for grade in range(1, number_of + 1)]
    largest = bound if full else min(bound, max(-(-total // number_of), total * loads[0] // sum(loads)))
    least = 1 if total - largest >= number_of - 1 else 0
    given, rest = [largest] + [least] * (number_of - 1), total - largest - least * (number_of - 1)
    while rest > 0:
        free = [i for i in range(1, number_of) if given[i] < largest] or [i for i in range(1, number_of) if given[i] < bound]
        pool, budget = sum([loads[i] for i in free]), rest
        for i in free:
            addition = min(bound - given[i], max(1, budget * loads[i] // pool), rest)
            given[i] = given[i] + addition
            rest = rest - addition
    return np.array(given)


def bell_draw(key, shape, scale, most, cuts=(), kind=jnp.bfloat16):
    values = scale * jax.random.normal(key, shape, jnp.float32)
    if cuts:
        values = values * block_levels(key, shape, cuts, -0.22, 0.18)
    return jnp.clip(values, -most, most).astype(kind)


def setup_inputs(seed: int = 0) -> dict:
    key_list = jax.random.split(jax.random.key(seed), 22)
    tokens = bell_draw(key_list[0], (BATCH, D), 1.0, 6.0, ((0, 32),))
    cache_latent = draw_cache_latent(jax.random.fold_in(key_list[21], 71), 0)
    cache_rope = bell_draw(key_list[2], (BATCH, ROT_DIM, LEN), 1.0, 6.0, ((0, 32),))
    lengths = draw_lengths(jax.random.fold_in(key_list[21], 71), 0)
    attn_gain = jnp.clip(1.0 + 0.18 * jax.random.normal(key_list[4], (D,), jnp.float32), 0.099609375, 1.8984375).astype(jnp.bfloat16)
    latent_gain = jnp.clip(1.0 + 0.18 * jax.random.normal(key_list[5], (LATENT,), jnp.float32), 0.099609375, 1.8984375).astype(jnp.bfloat16)
    post_attn_gain = jnp.clip(1.0 + 0.18 * jax.random.normal(key_list[6], (D,), jnp.float32), 0.099609375, 1.8984375).astype(jnp.bfloat16)
    ffn_gain = jnp.clip(1.0 + 0.18 * jax.random.normal(key_list[7], (D,), jnp.float32), 0.099609375, 1.8984375).astype(jnp.bfloat16)
    post_ffn_gain = jnp.clip(1.0 + 0.18 * jax.random.normal(key_list[8], (D,), jnp.float32), 0.099609375, 1.8984375).astype(jnp.bfloat16)
    w_query = bell_draw(key_list[9], (D, HEADS * KEY_DIM), D ** -0.5, 0.125, ((1, 4),))
    w_query_rot = bell_draw(key_list[10], (D, HEADS * ROT_DIM), D ** -0.5, 0.125, ((1, 4),))
    w_latent = bell_draw(key_list[11], (D, LATENT), D ** -0.5, 0.125, ((1, 4),))
    w_key_rot = bell_draw(key_list[12], (D, ROT_DIM), D ** -0.5, 0.125)
    w_key_up = bell_draw(key_list[13], (LATENT, HEADS, KEY_DIM), LATENT ** -0.5, 0.25, ((1, 4),))
    w_value_up = bell_draw(key_list[14], (LATENT, HEADS, VAL_DIM), LATENT ** -0.5, 0.25, ((1, 4),))
    w_out = bell_draw(key_list[15], (HEADS * VAL_DIM, D), (HEADS * VAL_DIM) ** -0.5, 0.125, ((0, 4),))
    route_logits = bell_draw(key_list[16], (BATCH, TOP_K), 1.0, 6.0, ((0, 8),), jnp.float32)
    routes_keys = jax.random.split(jax.random.fold_in(key_list[17], 1), BATCH // GROUP)
    routes_turns = jax.random.permutation(jax.random.fold_in(key_list[17], 3), BATCH // GROUP)
    routes = jax.vmap(lambda own, number: assign_block(jax.random.fold_in(key_list[17], 2), own, number, GROUP, EXPERTS, TOP_K, CAP, 2))(routes_keys, routes_turns).reshape((BATCH, TOP_K))
    w_gate = bell_draw(key_list[18], (EXPERTS, D, FF), 0.055, 0.3125, ((0, 8), (2, 4)))
    w_up = bell_draw(key_list[19], (EXPERTS, D, FF), 0.055, 0.3125, ((0, 8), (2, 4)))
    w_down = bell_draw(key_list[20], (EXPERTS, FF, D), FF ** -0.5, 0.125, ((0, 8), (1, 4)))
    return dict(tokens=tokens, cache_latent=cache_latent, cache_rope=cache_rope, lengths=lengths, attn_gain=attn_gain, latent_gain=latent_gain, post_attn_gain=post_attn_gain, ffn_gain=ffn_gain, post_ffn_gain=post_ffn_gain, w_query=w_query, w_query_rot=w_query_rot, w_latent=w_latent, w_key_rot=w_key_rot, w_key_up=w_key_up, w_value_up=w_value_up, w_out=w_out, route_logits=route_logits, routes=routes, w_gate=w_gate, w_up=w_up, w_down=w_down)


eps_norm = 1e-06
clamp_limit = 7.0
sigmoid_alpha = 1.702
theta_base = 10000.0

def rms_scale(values, gain):
    mean_square = lax.optimization_barrier(jnp.mean(values * values, axis=-1, keepdims=True))
    return values * lax.rsqrt(mean_square + eps_norm) * gain.astype(jnp.float32)

def rotate(values, positions):
    half = values.shape[-1] // 2
    freqs = theta_base ** (-jnp.arange(half, dtype=jnp.float32) / half)
    angles = positions[..., None] * freqs
    cosine = jnp.cos(angles)
    sine = jnp.sin(angles)
    first = values[..., :half]
    second = values[..., half:]
    return jnp.concatenate([first * cosine - second * sine, second * cosine + first * sine], axis=-1)

def reference(tokens, cache_latent, cache_rope, lengths, attn_gain, latent_gain, post_attn_gain, ffn_gain, post_ffn_gain, w_query, w_query_rot, w_latent, w_key_rot, w_key_up, w_value_up, w_out, route_logits, routes, w_gate, w_up, w_down):
    batch, width = tokens.shape
    latent_size, heads, key_size = w_key_up.shape
    rot_size = w_key_rot.shape[1]
    value_size = w_value_up.shape[2]
    span = cache_latent.shape[1]
    scale = (key_size + rot_size) ** (-0.5)
    token_values = tokens.astype(jnp.float32)
    normed = rms_scale(token_values, attn_gain).astype(jnp.bfloat16)
    query_plain = jnp.dot(normed, w_query, preferred_element_type=jnp.float32).astype(jnp.bfloat16)
    query_plain = query_plain.reshape(batch, heads, key_size)
    query_rotary = jnp.dot(normed, w_query_rot, preferred_element_type=jnp.float32).astype(jnp.bfloat16)
    query_rotary = query_rotary.reshape(batch, heads, rot_size)
    latent_raw = jnp.dot(normed, w_latent, preferred_element_type=jnp.float32).astype(jnp.bfloat16)
    key_raw = jnp.dot(normed, w_key_rot, preferred_element_type=jnp.float32).astype(jnp.bfloat16)
    new_latent = rms_scale(latent_raw.astype(jnp.float32), latent_gain).astype(jnp.bfloat16)
    positions = lengths.astype(jnp.float32)
    new_rope = rotate(key_raw.astype(jnp.float32), positions).astype(jnp.bfloat16)
    query_turned = rotate(query_rotary.astype(jnp.float32), positions[:, None]).astype(jnp.bfloat16)
    query_latent = jnp.einsum('bhn,chn->bhc', query_plain.astype(jnp.float32), w_key_up.astype(jnp.float32)).astype(jnp.bfloat16)

    def attend(pieces):
        q_lat, q_turn, latents, rotary, fresh_latent, fresh_rope, length = pieces
        latents_f = latents.astype(jnp.float32)
        scores = jnp.einsum('hc,pc->hp', q_lat.astype(jnp.float32), latents_f)
        scores = (scores + jnp.einsum('hr,rp->hp', q_turn.astype(jnp.float32), rotary.astype(jnp.float32))) * scale
        self_score = (lax.optimization_barrier(jnp.sum(q_lat.astype(jnp.float32) * fresh_latent.astype(jnp.float32)[None, :], axis=-1)) + lax.optimization_barrier(jnp.sum(q_turn.astype(jnp.float32) * fresh_rope.astype(jnp.float32)[None, :], axis=-1))) * scale
        valid = jnp.arange(span, dtype=jnp.int32) < length
        masked = jnp.where(valid[None, :], scores, -jnp.inf)
        highest = jnp.maximum(lax.optimization_barrier(jnp.max(masked, axis=-1)), self_score)
        raised = jnp.exp(masked - highest[:, None])
        raised_self = jnp.exp(self_score - highest)
        total = lax.optimization_barrier(jnp.sum(raised, axis=-1)) + raised_self
        probs = (raised / total[:, None]).astype(jnp.bfloat16)
        prob_self = (raised_self / total).astype(jnp.bfloat16)
        summed = jnp.einsum('hp,pc->hc', probs.astype(jnp.float32), latents_f)
        summed = summed + prob_self.astype(jnp.float32)[:, None] * fresh_latent.astype(jnp.float32)[None, :]
        return summed.astype(jnp.bfloat16)
    head_latent = lax.map(attend, (query_latent, query_turned, cache_latent, cache_rope, new_latent, new_rope, lengths))
    values = jnp.einsum('bhc,chv->bhv', head_latent.astype(jnp.float32), w_value_up.astype(jnp.float32)).astype(jnp.bfloat16)
    flat_values = values.reshape(batch, heads * value_size)
    group_cols = heads // N_TP * value_size
    attn = jnp.zeros((batch, width), jnp.float32)
    for section in range(N_TP):
        lower = section * group_cols
        partial_sum = jnp.dot(flat_values[:, lower:lower + group_cols], w_out[lower:lower + group_cols], preferred_element_type=jnp.float32).astype(jnp.bfloat16)
        attn = attn + partial_sum.astype(jnp.float32)
    attn = attn.astype(jnp.bfloat16)
    mixed = (token_values + rms_scale(attn.astype(jnp.float32), post_attn_gain)).astype(jnp.bfloat16)
    ffn_input = rms_scale(mixed.astype(jnp.float32), ffn_gain).astype(jnp.bfloat16)
    route_weights = jax.nn.softmax(route_logits, axis=-1)
    top_k = routes.shape[1]
    experts = w_gate.shape[0]
    hidden = w_gate.shape[2]
    n_blocks = batch // GROUP
    assigned = GROUP * top_k
    flat_routes = routes.reshape(n_blocks, assigned).astype(jnp.int32)
    onehot = (flat_routes[:, :, None] == jnp.arange(experts, dtype=jnp.int32)[None, None, :]).astype(jnp.int32)
    rank = lax.optimization_barrier(jnp.sum((jnp.cumsum(onehot, axis=1) - onehot) * onehot, axis=-1)).astype(jnp.int32)
    block_ids = jnp.broadcast_to(jnp.arange(n_blocks, dtype=jnp.int32)[:, None], (n_blocks, assigned))
    token_ids = (jnp.arange(assigned, dtype=jnp.int32) // top_k).astype(jnp.int32)
    rows_in = ffn_input.reshape(n_blocks, GROUP, width)
    gathered = rows_in[:, token_ids]
    slots = jnp.zeros((n_blocks, experts, CAP, width), jnp.bfloat16).at[block_ids, flat_routes, rank].set(gathered)
    block_hidden = hidden // N_TP

    def expert(pieces):
        rows, gate_weight, up_weight, down_weight = pieces
        flat = rows.reshape(-1, width)
        gate = jnp.minimum(jnp.dot(flat, gate_weight, preferred_element_type=jnp.float32), clamp_limit)
        upward = jnp.clip(jnp.dot(flat, up_weight, preferred_element_type=jnp.float32), -clamp_limit, clamp_limit)
        active = ((upward + 1.0) * gate * jax.nn.sigmoid(sigmoid_alpha * gate)).astype(jnp.bfloat16)
        total = jnp.zeros((flat.shape[0], width), jnp.float32)
        for section in range(N_TP):
            lower = section * block_hidden
            piece = jnp.dot(active[:, lower:lower + block_hidden], down_weight[lower:lower + block_hidden], preferred_element_type=jnp.float32).astype(jnp.bfloat16)
            total = total + piece.astype(jnp.float32)
        return total.astype(jnp.bfloat16).reshape(rows.shape)
    outputs = lax.map(expert, (jnp.moveaxis(slots, 1, 0), w_gate, w_up, w_down))
    picked = outputs[flat_routes, block_ids, rank].astype(jnp.float32).reshape(batch, top_k, width)
    moe = lax.optimization_barrier(jnp.sum(picked * route_weights[:, :, None], axis=1)).astype(jnp.bfloat16)
    result = (mixed.astype(jnp.float32) + rms_scale(moe.astype(jnp.float32), post_ffn_gain)).astype(jnp.bfloat16)
    return (result, new_latent, new_rope)
```

```python
import functools

import jax
import jax.numpy as jnp
import numpy as np
from jax import lax
from jax.experimental import pallas as pl
from jax.experimental.pallas import tpu as pltpu
from jax.sharding import PartitionSpec as P

eps_norm = 1e-06
clamp_limit = 7.0
sigmoid_alpha = 1.702
theta_base = 10000.0
MESH = pl.DeviceIdType.MESH
F32 = jnp.float32
BF16 = jnp.bfloat16
SUB = 8
LANES = 128


def rms_scale(values, gain):
    mean_square = jnp.mean(values * values, axis=-1, keepdims=True)
    return values * lax.rsqrt(mean_square + eps_norm) * gain


def turn(values, cosine, sine):
    half = values.shape[-1] // 2
    swapped = jnp.concatenate([values[:, half:], values[:, :half]], axis=1)
    return values * cosine + swapped * sine


def dot(a, b):
    return jnp.dot(a, b, preferred_element_type=F32)


def dot_nt(a, b):
    return lax.dot_general(a, b, (((1,), (1,)), ((), ())), preferred_element_type=F32)


def remote(src, dst, send_sem, recv_sem, where):
    return pltpu.make_async_remote_copy(
        src_ref=src,
        dst_ref=dst,
        send_sem=send_sem,
        recv_sem=recv_sem,
        device_id=where,
        device_id_type=MESH,
    )


def half_rows(values):
    return lax.broadcasted_iota(jnp.int32, values.shape, 0) < SUB // 2


def join_halves(upper, lower):
    return jnp.where(half_rows(upper), upper, pltpu.roll(lower, SUB // 2, 0))


def join_ends(upper, lower):
    return jnp.where(half_rows(upper), pltpu.roll(upper, SUB // 2, 0), lower)


def layout(T, R, LH):
    H = T * LH
    half = R // 2

    def packed(s, b):
        if b < SUB:
            return s * SUB + b
        return T * SUB + (s // 2) * SUB + (s % 2) * (SUB // 2) + b - SUB

    def query_slot(s, h, b):
        base = s * LH * R
        if b < SUB:
            return base + h * SUB + b
        return base + LH * SUB + (h // 2) * SUB + (h % 2) * (SUB // 2) + b - SUB

    to_seq = np.zeros((R * H, R * H))
    to_seq_wide = np.zeros((R * H, 2 * SUB * H))
    for b in range(R):
        for s in range(T):
            for h in range(LH):
                to_seq[b * H + s * LH + h, query_slot(s, h, b)] = 1
                to_seq_wide[b * H + s * LH + h, (s * LH + h) * 2 * SUB + b] = 1
    to_head = np.zeros((half * H, half * H))
    for g in range(T):
        for h in range(LH):
            for b in range(half):
                to_head[(g * LH + h) * half + b, b * H + g * LH + h] = 1
    to_value = np.zeros((LH * T * R, LH * T * R))
    for s in range(T):
        for h in range(LH):
            for b in range(R):
                src = ((b // half) * T + s) * LH * half + h * half + b % half
                to_value[h * T * R + packed(s, b), src] = 1
    spread = np.zeros((T * R, T * R))
    own_natural = np.zeros((T * 2 * SUB, T * R))
    own_packed = np.zeros((T * 2 * SUB, T * R))
    for s in range(T):
        for b in range(R):
            spread[packed(s, b), s * R + b] = 1
            own_natural[s * 2 * SUB + b, s * R + b] = 1
            own_packed[s * 2 * SUB + b, packed(s, b)] = 1
    parts = [to_seq, to_seq_wide, to_head, to_value, spread, own_natural, own_packed]
    width = max(p.shape[1] for p in parts)
    rows, places = 0, []
    for p in parts:
        places.append((rows, p.shape[0], p.shape[1]))
        rows += -(-p.shape[0] // 16) * 16
    table = np.zeros((rows, width), np.float32)
    for p, (row, n, m) in zip(parts, places):
        table[row : row + n, :m] = p
    return table, tuple(places)


def kernel(
    cfg,
    lengths,
    tokens,
    attn_gain,
    latent_gain,
    post_attn_gain,
    ffn_gain,
    post_ffn_gain,
    routes_t,
    logits_t,
    table_h,
    cache_h,
    rope_h,
    wq_h,
    wqr_h,
    wl_h,
    wkr_h,
    wku_h,
    wvu_h,
    wo_h,
    wg_h,
    wu_h,
    wd_h,
    out_result,
    out_latent,
    out_rope,
    table,
    cache,
    rope,
    wall,
    wkr,
    wku,
    wvu,
    wo,
    wgu,
    wd,
    xg,
    rows_all,
    gains,
    qsend,
    qrecv,
    qs,
    qt,
    nlat,
    nrope,
    hl,
    hsend,
    hrecv,
    asend,
    arecv,
    srecv,
    mxsend,
    mxrecv,
    sl,
    xr,
    part,
    s1,
    xsend,
    xrecv,
    rsend,
    ret,
    msend,
    mrecv,
    ku3,
    vu3,
    wide,
    sc,
    pb,
    w_sem,
    tp_send,
    tp_recv,
    d_send,
    d_recv,
    x_send,
    x_recv,
    sib_send,
    sib_recv,
    s1_send,
    s1_recv,
    rx_send,
    rx_recv,
    ret_send,
    ret_recv,
):
    T, EP, R, LH, CP, scale, places = cfg
    H = T * LH
    t = lax.axis_index("tp")
    e = lax.axis_index("ep")
    C = wku.shape[0]
    KD = wku.shape[1] // LH
    RD = wkr.shape[0]
    VD = wvu.shape[1] // LH
    D, WA = wall.shape
    F = wd.shape[0]
    LC = WA - LH * KD - LH * RD
    Q = D // T
    N = T * R
    RP = 2 * SUB
    S = EP * CP
    SPAN = cache.shape[1]
    HALF = R // 2
    HR = HALF * LH
    FOLD = D // 2
    pairs = T // 2
    sib = t + 1 - 2 * lax.rem(t, 2)

    def one_hot(i):
        row, n, m = places[i]
        return table[row : row + n, :m]

    def swap(k):
        other = e
        bit = 1
        while bit < EP:
            if k & bit:
                other = other + bit - 2 * bit * lax.rem(lax.div(e, bit), 2)
            bit *= 2
        return other

    loads = {}
    for i, (name, copies) in enumerate(
        [
            (
                "wall",
                [
                    (wq_h, wall.at[:, : LH * KD]),
                    (wqr_h, wall.at[:, LH * KD : LH * KD + LH * RD]),
                    (wl_h, wall.at[:, LH * KD + LH * RD :]),
                ],
            ),
            ("wkr", [(wkr_h, wkr)]),
            ("wku", [(wku_h, ku3)]),
            ("wvu", [(wvu_h, vu3)]),
            ("wo", [(wo_h, wo)]),
            ("wgu", [(wg_h.at[0], wgu.at[:, :F]), (wu_h.at[0], wgu.at[:, F:])]),
            ("wd", [(wd_h.at[0], wd)]),
            ("table", [(table_h, table)]),
            ("cache", [(cache_h.at[b], cache.at[b]) for b in range(R)]),
            ("rope", [(rope_h, rope)]),
        ]
    ):
        loads[name] = (i, copies)
    whole = {
        "wall": wall,
        "wkr": wkr,
        "wku": ku3,
        "wvu": vu3,
        "wo": wo,
        "wgu": wgu,
        "wd": wd,
        "table": table,
        "cache": cache,
        "rope": rope,
    }

    def fetch(name):
        i, copies = loads[name]
        for src, dst in copies:
            pltpu.make_async_copy(src, dst, w_sem.at[i]).start()

    def arrive(name):
        i, _ = loads[name]
        pltpu.make_async_copy(whole[name], whole[name], w_sem.at[i]).wait()

    for name in ("wku", "wkr", "wall", "table"):
        fetch(name)

    barrier = pltpu.get_barrier_semaphore()
    for k in range(1, T):
        pl.semaphore_signal(
            barrier, inc=1, device_id={"tp": lax.rem(t + k, T)}, device_id_type=MESH
        )
    for k in range(1, EP):
        pl.semaphore_signal(
            barrier, inc=1, device_id={"ep": swap(k)}, device_id_type=MESH
        )

    def gain(ref):
        return ref[...].astype(F32)[None, :]

    def by_head_columns(source, target):
        size = source.shape[2]
        wide[...] = source[...].astype(F32).reshape(C * LH, size)
        for h in range(LH):
            target[:, h * size : (h + 1) * size] = wide[pl.ds(h, C, stride=LH), :].astype(BF16)

    def settle_recv(ref, sem):
        remote(ref, ref, sem, sem, {"tp": sib}).wait_recv()

    def settle_send(ref, sem):
        remote(ref, ref, sem, sem, {"tp": sib}).wait_send()

    def gather_tp(phase, src, dst):
        for k in range(1, T):
            peer = lax.rem(t + k, T)
            remote(
                src, dst.at[t], tp_send.at[phase], tp_recv.at[phase], {"tp": peer}
            ).start()

    def scatter_tp(phase, src, dst):
        for k in range(1, T):
            peer = lax.rem(t + k, T)
            remote(
                src.at[peer], dst.at[t], tp_send.at[phase], tp_recv.at[phase], {"tp": peer}
            ).start()
        dst[t] = src[t]

    sent_tp = []

    def finish_tp(phase, dst):
        settle_recv(dst.at[pl.ds(0, T - 1)], tp_recv.at[phase])
        sent_tp.append((phase, dst))

    token_values = jnp.concatenate(
        [tokens[...].astype(F32), jnp.zeros((RP - R, D), F32)], axis=0
    )
    left, right = token_values[SUB:, :FOLD], token_values[SUB:, FOLD:]
    xg[t] = jnp.concatenate(
        [token_values[:SUB], join_halves(left, right)], axis=1
    ).astype(BF16)
    pl.semaphore_wait(barrier, T - 1 + EP - 1)

    gather_tp(0, xg.at[t], xg)
    fetch("cache")
    fetch("rope")
    own_normed = rms_scale(token_values, gain(attn_gain)).astype(BF16)
    for i, ref in enumerate((post_attn_gain, ffn_gain)):
        gains[i : i + 1, :] = gain(ref)
    half = RD // 2
    lane = lax.broadcasted_iota(jnp.int32, (RP, RD), 1)
    row = lax.broadcasted_iota(jnp.int32, (RP, RD), 0)
    freqs = jnp.zeros((RP, RD), F32)
    for i in range(half):
        hit = (lane == i) | (lane == i + half)
        freqs = jnp.where(hit, np.float32(theta_base ** (-i / half)), freqs)
    positions = jnp.zeros((RP, RD), jnp.int32)
    for b in range(R):
        positions = jnp.where(row == b, lengths[b], positions)
    angles = positions.astype(F32) * freqs
    cosine = jnp.cos(angles)
    sine = jnp.sin(angles)
    sine = jnp.where(lane < half, -sine, sine)
    arrive("wku")
    by_head_columns(ku3, wku)
    arrive("wkr")
    key_raw = dot_nt(own_normed, wkr[...]).astype(BF16).astype(F32)
    new_rope = turn(key_raw, cosine, sine).astype(BF16)
    nrope[...] = new_rope.astype(F32)
    out_rope[...] = new_rope[:R]
    arrive("wall")
    arrive("table")
    finish_tp(0, xg)

    blocks = [xg[s, :, :D].astype(F32) for s in range(T)]
    for p in range(pairs):
        first = xg[2 * p, :, D:].astype(F32)
        second = xg[2 * p + 1, :, D:].astype(F32)
        blocks.append(
            jnp.concatenate([join_halves(first, second), join_ends(first, second)], axis=1)
        )
    rows = jnp.concatenate(blocks, axis=0)
    rows_all[...] = rows.astype(BF16)
    row_square = jnp.sum(rows * rows, axis=1, keepdims=True)
    normed = (rows * lax.rsqrt(row_square * (1.0 / D) + eps_norm) * gain(attn_gain)).astype(BF16)
    projected = dot(normed, wall[...])
    plain = projected[:, : LH * KD].astype(BF16)
    extra = projected[:, LH * KD :]
    lifted = [
        dot_nt(plain[:, h * KD : (h + 1) * KD], wku[:, h * KD : (h + 1) * KD])
        for h in range(LH)
    ]
    base = LH * C
    fold_base = base + (LH // 2) * C
    ROT = LH * RD
    for s in range(T):
        join = join_halves if s % 2 == 0 else join_ends
        top = slice(s * SUB, (s + 1) * SUB)
        rest = slice(T * SUB + (s // 2) * SUB, T * SUB + (s // 2 + 1) * SUB)
        for h in range(LH):
            qsend[s, :, h * C : (h + 1) * C] = lifted[h][top].astype(BF16)
        for h in range(0, LH, 2):
            at = base + (h // 2) * C
            qsend[s, :, at : at + C] = join(lifted[h][rest], lifted[h + 1][rest]).astype(BF16)
        at = fold_base
        qsend[s, :, at : at + ROT + LC] = extra[top].astype(BF16)
        at += ROT + LC
        tail = extra[rest]
        qsend[s, :, at : at + ROT // 2] = join(
            tail[:, : ROT // 2], tail[:, ROT // 2 : ROT]
        ).astype(BF16)
        at += ROT // 2
        tail_latent = tail[:, ROT:]
        qsend[s, :, at : at + LC] = join(tail_latent, tail_latent).astype(BF16)
    scatter_tp(1, qsend, qrecv)
    for name in ("wvu", "wo", "wgu", "wd"):
        fetch(name)
    finish_tp(1, qrecv)

    at = fold_base
    latent_raw = jnp.concatenate(
        [
            jnp.concatenate(
                [
                    qrecv[s, :, at + ROT : at + ROT + LC],
                    qrecv[s, :, at + ROT + LC + ROT // 2 :],
                ],
                axis=0,
            )
            for s in range(T)
        ],
        axis=1,
    ).astype(F32)
    new_latent = rms_scale(latent_raw, gain(latent_gain)).astype(BF16)
    out_latent[...] = new_latent[:R]
    nlat[...] = new_latent.astype(F32)
    stacked = jnp.concatenate(
        [
            qrecv[s, :, i * C : (i + 1) * C]
            for s in range(T)
            for i in range(LH + LH // 2)
        ],
        axis=0,
    )
    qs[...] = dot(one_hot(0), stacked).astype(BF16).reshape(R, H, C)
    turned = []
    for s in range(T):
        head = qrecv[s, :, at : at + ROT].astype(F32)
        fold = qrecv[s, :, at + ROT + LC : at + ROT + LC + ROT // 2].astype(F32)
        tail = jnp.concatenate([fold, pltpu.roll(fold, SUB // 2, 0)], axis=1)
        rotary = jnp.concatenate([head, tail], axis=0)
        for h in range(LH):
            turned.append(turn(rotary[:, h * RD : (h + 1) * RD], cosine, sine).astype(BF16))
    qt[...] = dot(one_hot(1), jnp.concatenate(turned, axis=0)).astype(BF16).reshape(R, H, RD)

    arrive("cache")
    arrive("rope")
    position = lax.broadcasted_iota(jnp.int32, (H, SPAN), 1)
    for part_of in range(2):
        members = range(part_of * HALF, (part_of + 1) * HALF)
        for b in members:
            scores = (dot_nt(qs[b], cache[b]) + dot(qt[b], rope[b])) * scale
            sc[b] = jnp.where(position < lengths[b], scores, -jnp.inf)
        prob_own = {}
        for b in members:
            own = (
                jnp.sum(qs[b].astype(F32) * nlat[b : b + 1, :], axis=1, keepdims=True)
                + jnp.sum(qt[b].astype(F32) * nrope[b : b + 1, :], axis=1, keepdims=True)
            ) * scale
            masked = sc[b]
            highest = jnp.maximum(jnp.max(masked, axis=1, keepdims=True), own)
            raised = jnp.exp(masked - highest)
            raised_own = jnp.exp(own - highest)
            inverse = 1.0 / (jnp.sum(raised, axis=1, keepdims=True) + raised_own)
            pb[b] = (raised * inverse).astype(BF16)
            prob_own[b] = (raised_own * inverse).astype(BF16).astype(F32)
        for b in members:
            hl[b] = (dot(pb[b], cache[b]) + prob_own[b] * nlat[b : b + 1, :]).astype(BF16)
        attended = hl[part_of * HALF : (part_of + 1) * HALF].reshape(HALF * H, C)
        hsend[part_of] = dot(one_hot(2), attended).astype(BF16).reshape(T, HR, C)
        scatter_tp(2 + part_of, hsend.at[part_of], hrecv.at[part_of])

    arrive("wvu")
    by_head_columns(vu3, wvu)
    arrive("wo")
    slot_shift = CP.bit_length() - 1
    s_sub = lax.broadcasted_iota(jnp.int32, (S, N), 0)
    e_sub = (s_sub >> slot_shift) ^ e
    c_sub = (s_sub & (CP - 1)).astype(F32)
    gi = lax.broadcasted_iota(jnp.int32, (N, N), 0)
    gj = lax.broadcasted_iota(jnp.int32, (N, N), 1)
    upper = (gi < gj).astype(F32).astype(BF16)
    lg = logits_t[...]
    lg = jnp.exp(lg - jnp.max(lg, axis=0, keepdims=True))
    weights = lg / jnp.sum(lg, axis=0, keepdims=True)
    count = jnp.zeros((S, N), F32)
    weighted = jnp.zeros((S, N), F32)
    for k in range(routes_t.shape[0]):
        hit = routes_t[k : k + 1, :] == e_sub
        count = jnp.where(hit, 1.0, count)
        weighted = jnp.where(hit, weights[k : k + 1, :], weighted)
    rank = dot(count.astype(BF16), upper)
    taken = rank == c_sub
    weighted = jnp.where(taken, weighted, 0.0)
    weighted_hi = weighted.astype(BF16)
    weighted_lo = (weighted - weighted_hi.astype(F32)).astype(BF16)
    combine_hi = dot_nt(one_hot(5), weighted_hi).astype(BF16)
    combine_lo = dot_nt(one_hot(5), weighted_lo).astype(BF16)
    dispatch = dot_nt(jnp.where(taken, count, 0.0).astype(BF16), one_hot(4)).astype(BF16)

    finish_tp(2, hrecv.at[0])
    finish_tp(3, hrecv.at[1])
    heads = dot(one_hot(3), hrecv[...].reshape(2 * T * HR, C)).astype(BF16)
    values = jnp.concatenate(
        [
            dot(heads[h * N : (h + 1) * N], wvu[:, h * VD : (h + 1) * VD]).astype(BF16)
            for h in range(LH)
        ],
        axis=1,
    )
    for q in range(T):
        asend[q] = dot(values, wo[:, q * Q : (q + 1) * Q]).astype(BF16)
    scatter_tp(4, asend, arecv)
    finish_tp(4, arecv)
    quarter_lanes = pl.ds(pl.multiple_of(t * Q, Q), Q)
    attn = arecv[0].astype(F32)
    for s in range(1, T):
        attn = attn + arecv[s].astype(F32)
    attn = attn.astype(BF16).astype(F32)
    own_tokens = rows_all[:, quarter_lanes].astype(F32)
    scaled = attn * gains[0:1, quarter_lanes]

    def row_sum(v):
        return jnp.sum(v, axis=1, keepdims=True)

    at_lane = lax.broadcasted_iota(jnp.int32, (N, LANES), 1)
    sums = jnp.where(at_lane == 0, row_sum(attn * attn), 0.0)
    sums = jnp.where(at_lane == 1, row_sum(own_tokens * scaled), sums)
    sums = jnp.where(at_lane == 2, row_sum(scaled * scaled), sums)
    sums = jnp.concatenate([sums, jnp.zeros((LANES - N, LANES), F32)], axis=0)
    srecv[t] = sums.T[:SUB]
    gather_tp(5, srecv.at[t], srecv)
    finish_tp(5, srecv)
    totals = srecv[0]
    for s in range(1, T):
        totals = totals + srecv[s]
    totals = jnp.concatenate([totals, jnp.zeros((LANES - SUB, LANES), F32)], axis=0).T[:N]
    inverse = lax.rsqrt(totals[:, 0:1] * (1.0 / D) + eps_norm)
    mixed = (own_tokens + scaled * inverse).astype(BF16)
    square = row_square + 2.0 * inverse * totals[:, 1:2] + inverse * inverse * totals[:, 2:3]
    square = jnp.maximum(square, 0.0)
    ffn_rows = (
        mixed.astype(F32)
        * lax.rsqrt(square * (1.0 / D) + eps_norm)
        * gains[1:2, quarter_lanes]
    ).astype(BF16)
    sl[...] = dot(dispatch, ffn_rows).astype(BF16).reshape(EP, CP, Q)
    order = sorted(range(1, EP), key=lambda k: (-k.bit_length(), k))
    far = EP // 2
    chunks = [range(far, EP), range(0, far)]
    for k in order:
        remote(sl.at[k], xr.at[t, k], d_send.at[0], d_recv.at[k], {"ep": swap(k)}).start()
    xr[t, 0] = sl[0]
    mxsend[...] = dot(one_hot(6), mixed).astype(BF16).reshape(T, RP, Q)
    scatter_tp(6, mxsend, mxrecv)

    def to_peer(k, j):
        return remote(
            xr.at[t, k],
            xr.at[t, k],
            x_send.at[0],
            x_recv.at[k, j],
            {"tp": lax.rem(t + 2 * j, T)},
        )

    def to_sib(c, quarter, k):
        return remote(
            xr.at[quarter, k], xr.at[quarter, k], sib_send.at[0], sib_recv.at[c], {"tp": sib}
        )

    for c, chunk in ((1, [0]), (0, order[:far]), (1, order[far:])):
        for k in chunk:
            if k:
                settle_recv(xr.at[t, k], d_recv.at[k])
            for j in range(1, pairs):
                to_peer(k, j).start()
            to_sib(c, t, k).start()

    def relay(c):
        for k in [k for k in [0] + order if (k < far) == (c == 1)]:
            for j in range(1, pairs):
                settle_recv(xr.at[t, k], x_recv.at[k, j])
                to_sib(c, lax.rem(t + T - 2 * j, T), k).start()

    def experts(c):
        lo = chunks[c][0]
        settle_recv(xr.at[pl.ds(0, pairs), pl.ds(lo, far)], sib_recv.at[c])
        block = jnp.concatenate(
            [xr[q, lo : lo + far].reshape(far * CP, Q) for q in range(T)], axis=1
        )
        both = dot(block, wgu[...])
        gate = jnp.minimum(both[:, :F], clamp_limit)
        upward = jnp.clip(both[:, F:], -clamp_limit, clamp_limit)
        active = (upward + 1.0) * gate * (1.0 / (1.0 + jnp.exp(-sigmoid_alpha * gate)))
        active = active.astype(BF16)

        def down(quarter):
            cols = pl.ds(pl.multiple_of(quarter * Q, Q), Q)
            part[quarter, lo : lo + far] = (
                dot(active, wd[:, cols]).astype(BF16).reshape(far, CP, Q)
            )

        for j in range(pairs - 1, -1, -1):
            quarter = lax.rem(sib + 2 * j, T)
            down(quarter)
            remote(
                part.at[quarter, pl.ds(lo, far)],
                s1.at[quarter, pl.ds(lo, far)],
                s1_send.at[0],
                s1_recv.at[c, j],
                {"tp": sib},
            ).start()
        for j in range(pairs - 1, -1, -1):
            down(lax.rem(t + 2 * j, T))

    def reduce_across(c):
        lo = chunks[c][0]
        for j in range(pairs - 1, 0, -1):
            quarter = lax.rem(t + 2 * j, T)
            settle_recv(s1.at[quarter, pl.ds(lo, far)], s1_recv.at[c, j])
            for k in [k for k in order + [0] if k in chunks[c]]:
                both = part[quarter, k].astype(F32) + s1[quarter, k].astype(F32)
                xsend[j, k] = both.astype(BF16)
                remote(
                    xsend.at[j, k], xrecv.at[j, k], rx_send.at[0], rx_recv.at[k, j], {"tp": quarter}
                ).start()

    def send_back(c):
        lo = chunks[c][0]
        settle_recv(s1.at[t, pl.ds(lo, far)], s1_recv.at[c, 0])
        for k in [k for k in order + [0] if k in chunks[c]]:
            total = part[t, k].astype(F32) + s1[t, k].astype(F32)
            for j in range(1, pairs):
                settle_recv(xrecv.at[j, k], rx_recv.at[k, j])
                total = total + xrecv[j, k].astype(F32)
            if k:
                rsend[k] = total.astype(BF16)
                remote(
                    rsend.at[k], ret.at[k], ret_send.at[0], ret_recv.at[0], {"ep": swap(k)}
                ).start()
            else:
                ret[0] = total.astype(BF16)

    relay(0)
    relay(1)
    arrive("wgu")
    arrive("wd")
    experts(0)
    reduce_across(0)
    experts(1)
    reduce_across(1)
    send_back(0)
    send_back(1)
    settle_recv(ret.at[pl.ds(1, EP - 1)], ret_recv.at[0])
    returned = ret[...].reshape(S, Q)
    moe_part = dot(combine_hi, returned) + dot(combine_lo, returned)
    msend[...] = moe_part.astype(BF16).reshape(T, RP, Q)
    scatter_tp(7, msend, mrecv)
    finish_tp(6, mxrecv)
    finish_tp(7, mrecv)
    moe = jnp.concatenate([mrecv[s] for s in range(T)], axis=1).astype(F32)
    mixed_own = jnp.concatenate([mxrecv[s] for s in range(T)], axis=1).astype(F32)
    out_result[...] = (mixed_own + rms_scale(moe, gain(post_ffn_gain))).astype(BF16)[:R]

    for phase, dst in sent_tp:
        settle_send(dst.at[pl.ds(0, T - 1)], tp_send.at[phase])
    settle_send(sl.at[pl.ds(1, EP - 1)], d_send.at[0])
    if pairs > 1:
        settle_send(xr.at[pl.ds(0, pairs - 1)], x_send.at[0])
        settle_send(xsend.at[pl.ds(1, pairs - 1)], rx_send.at[0])
    settle_send(xr.at[pl.ds(0, pairs)], sib_send.at[0])
    settle_send(part.at[pl.ds(0, pairs)], s1_send.at[0])
    settle_send(rsend.at[pl.ds(1, EP - 1)], ret_send.at[0])


def hand_over(result, latent, rope, out_result, out_latent, out_rope):
    out_result[...] = result[...]
    out_latent[...] = latent[...]
    out_rope[...] = rope[...]


def body(
    tokens,
    cache_latent,
    cache_rope,
    lengths,
    attn_gain,
    latent_gain,
    post_attn_gain,
    ffn_gain,
    post_ffn_gain,
    w_query,
    w_query_rot,
    w_latent,
    w_key_rot,
    w_key_up,
    w_value_up,
    w_out,
    route_logits,
    routes,
    w_gate,
    w_up,
    w_down,
):
    R, D = tokens.shape
    T = lax.axis_size("tp")
    EP = lax.axis_size("ep")
    C, LH, KD = w_key_up.shape
    RD = w_key_rot.shape[1]
    VD = w_value_up.shape[2]
    H = T * LH
    K = routes.shape[1]
    scale = (KD + RD) ** (-0.5)
    RP = 2 * SUB
    assert R == SUB + SUB // 2 and T % 2 == 0 and LH % 2 == 0
    assert EP & (EP - 1) == 0 and T * R <= LANES
    cap = (R * T * K + EP - 1) // EP + 1
    CP = 16
    while CP < cap:
        CP *= 2
    Q = D // T
    F = w_gate.shape[2]
    LC = w_latent.shape[1]
    SPAN = cache_latent.shape[1]
    N = T * R
    table, places = layout(T, R, LH)

    vm = pl.BlockSpec(memory_space=pltpu.VMEM)
    hbm = pl.BlockSpec(memory_space=pl.ANY)
    dma = pltpu.SemaphoreType.DMA
    pairs = T // 2
    ROT = LH * RD
    QW = (LH + LH // 2) * C + ROT + LC + ROT // 2 + LC

    def v(*shape, dtype=BF16):
        return pltpu.VMEM(shape, dtype)

    cfg = (T, EP, R, LH, CP, scale, places)
    outs = pl.pallas_call(
        functools.partial(kernel, cfg),
        out_shape=(
            jax.ShapeDtypeStruct((R, D), BF16),
            jax.ShapeDtypeStruct((R, C), BF16),
            jax.ShapeDtypeStruct((R, RD), BF16),
        ),
        in_specs=[pl.BlockSpec(memory_space=pltpu.SMEM)] + [vm] * 8 + [hbm] * 13,
        out_specs=(vm, vm, vm),
        scratch_shapes=[
            v(*table.shape),
            v(R, SPAN, C),
            v(R, RD, SPAN),
            v(D, LH * KD + ROT + LC),
            v(RD, D),
            v(C, LH * KD),
            v(C, LH * VD),
            v(LH * VD, D),
            v(D, 2 * F),
            v(F, D),
            v(T, SUB, D + D // 2),
            v(N, D),
            v(SUB, D, dtype=F32),
            v(T, SUB, QW),
            v(T, SUB, QW),
            v(R, H, C),
            v(R, H, RD),
            v(RP, C, dtype=F32),
            v(RP, RD, dtype=F32),
            v(R, H, C),
            v(2, T, R // 2 * LH, C),
            v(2, T, R // 2 * LH, C),
            v(T, N, Q),
            v(T, N, Q),
            v(T, SUB, LANES, dtype=F32),
            v(T, RP, Q),
            v(T, RP, Q),
            v(EP, CP, Q),
            v(T, EP, CP, Q),
            v(T, EP, CP, Q),
            v(T, EP, CP, Q),
            v(pairs, EP, CP, Q),
            v(pairs, EP, CP, Q),
            v(EP, CP, Q),
            v(EP, CP, Q),
            v(T, RP, Q),
            v(T, RP, Q),
            v(C, LH, KD),
            v(C, LH, VD),
            v(C * LH, KD, dtype=F32),
            v(R, H, SPAN, dtype=F32),
            v(R, H, SPAN),
            dma((10,)),
            dma((8,)),
            dma((8,)),
            dma((1,)),
            dma((EP,)),
            dma((1,)),
            dma((EP, pairs)),
            dma((1,)),
            dma((2,)),
            dma((1,)),
            dma((2, pairs)),
            dma((1,)),
            dma((EP, pairs)),
            dma((1,)),
            dma((1,)),
        ],
        compiler_params=pltpu.CompilerParams(
            collective_id=0, has_side_effects=True, vmem_limit_bytes=60 * 1024 * 1024
        ),
    )(
        lengths,
        tokens,
        attn_gain,
        latent_gain,
        post_attn_gain,
        ffn_gain,
        post_ffn_gain,
        routes.T,
        route_logits.T,
        jnp.asarray(table, BF16),
        cache_latent,
        cache_rope,
        w_query,
        w_query_rot,
        w_latent,
        w_key_rot.T,
        w_key_up,
        w_value_up,
        w_out,
        w_gate,
        w_up,
        w_down,
    )
    return pl.pallas_call(
        hand_over,
        out_shape=tuple(jax.ShapeDtypeStruct(o.shape, o.dtype) for o in outs),
        in_specs=[vm] * 3,
        out_specs=(vm, vm, vm),
    )(*outs)


def solution(mesh):
    return jax.shard_map(
        body,
        mesh=mesh,
        in_specs=(
            P(("ep", "tp"), None),
            P(("ep", "tp"), None, None),
            P(("ep", "tp"), None, None),
            P(("ep", "tp")),
            P(),
            P(),
            P(),
            P(),
            P(),
            P(None, "tp"),
            P(None, "tp"),
            P(None, "tp"),
            P(),
            P(None, "tp", None),
            P(None, "tp", None),
            P("tp", None),
            P("ep", None),
            P("ep", None),
            P("ep", None, "tp"),
            P("ep", None, "tp"),
            P("ep", "tp", None),
        ),
        out_specs=(P(("ep", "tp"), None), P(("ep", "tp"), None), P(("ep", "tp"), None)),
        check_vma=False,
    )
```

```python
import functools

import jax
import jax.numpy as jnp
import numpy as np
from jax import lax
from jax.experimental import pallas as pl
from jax.experimental.pallas import tpu as pltpu
from jax.sharding import PartitionSpec as P

eps_norm = 1e-06
clamp_limit = 7.0
sigmoid_alpha = 1.702
theta_base = 10000.0
MESH = pl.DeviceIdType.MESH
F32 = jnp.float32
BF16 = jnp.bfloat16
SUB = 8
LANES = 128


def rms_scale(values, gain):
    mean_square = jnp.mean(values * values, axis=-1, keepdims=True)
    return values * lax.rsqrt(mean_square + eps_norm) * gain


def turn(values, cosine, sine):
    half = values.shape[-1] // 2
    swapped = jnp.concatenate([values[:, half:], values[:, :half]], axis=1)
    return values * cosine + swapped * sine


def dot(a, b):
    return jnp.dot(a, b, preferred_element_type=F32)


def dot_nt(a, b):
    return lax.dot_general(a, b, (((1,), (1,)), ((), ())), preferred_element_type=F32)


def remote(src, dst, send_sem, recv_sem, where):
    return pltpu.make_async_remote_copy(
        src_ref=src,
        dst_ref=dst,
        send_sem=send_sem,
        recv_sem=recv_sem,
        device_id=where,
        device_id_type=MESH,
    )


def half_rows(values):
    return lax.broadcasted_iota(jnp.int32, values.shape, 0) < SUB // 2


def join_halves(upper, lower):
    return jnp.where(half_rows(upper), upper, pltpu.roll(lower, SUB // 2, 0))


def join_ends(upper, lower):
    return jnp.where(half_rows(upper), pltpu.roll(upper, SUB // 2, 0), lower)


def layout(T, R, LH, chunks, FT, REST, QL):
    H = T * LH
    half = R // 2

    def packed(s, b):
        if b < SUB:
            return s * SUB + b
        return T * SUB + (s // 2) * SUB + (s % 2) * (SUB // 2) + b - SUB

    def query_slot(s, h, b):
        base = s * LH * R
        if b < SUB:
            return base + h * SUB + b
        return base + LH * SUB + (h // 2) * SUB + (h % 2) * (SUB // 2) + b - SUB

    to_seq = np.zeros((R * H, R * H))
    to_seq_wide = np.zeros((R * H, 2 * SUB * H))
    for b in range(R):
        for s in range(T):
            for h in range(LH):
                to_seq[b * H + s * LH + h, query_slot(s, h, b)] = 1
                to_seq_wide[b * H + s * LH + h, (s * LH + h) * 2 * SUB + b] = 1
    to_head = np.zeros((half * H, half * H))
    for g in range(T):
        for h in range(LH):
            for b in range(half):
                to_head[(g * LH + h) * half + b, b * H + g * LH + h] = 1
    to_value = np.zeros((LH * T * R, LH * T * R))
    for s in range(T):
        for h in range(LH):
            for b in range(R):
                src = ((b // half) * T + s) * LH * half + h * half + b % half
                to_value[h * T * R + packed(s, b), src] = 1
    spread = np.zeros((T * R, T * R))
    own_natural = np.zeros((T * 2 * SUB, T * R))
    own_packed = np.zeros((T * 2 * SUB, T * R))
    for s in range(T):
        for b in range(R):
            spread[packed(s, b), s * R + b] = 1
            own_natural[s * 2 * SUB + b, s * R + b] = 1
            own_packed[s * 2 * SUB + b, packed(s, b)] = 1
    groups, slots = [], []
    for lo, n in chunks:
        for k in range(n):
            groups += [lo + k] * (FT * SUB)
            slots += range(FT * SUB)
        for k in range(n if REST else 0):
            groups += [lo + k] * SUB
            slots += [FT * SUB] * QL + [-1] * (SUB - QL)
    group_of = np.repeat(np.array(groups)[:, None], T * R, 1)
    slot_of = np.repeat(np.array(slots)[:, None], T * R, 1)
    parts = [to_seq, to_seq_wide, to_head, to_value, spread, own_natural, own_packed]
    parts += [group_of, slot_of]
    width = max(p.shape[1] for p in parts)
    rows, places = 0, []
    for p in parts:
        places.append((rows, p.shape[0], p.shape[1]))
        rows += -(-p.shape[0] // 16) * 16
    table = np.zeros((rows, width), np.float32)
    for p, (row, n, m) in zip(parts, places):
        table[row : row + n, :m] = p
    return table, tuple(places)


def kernel(
    cfg,
    lengths,
    tokens,
    attn_gain,
    latent_gain,
    post_attn_gain,
    ffn_gain,
    post_ffn_gain,
    routes_t,
    logits_t,
    table_h,
    cache_h,
    rope_h,
    wq_h,
    wqr_h,
    wl_h,
    wkr_h,
    wku_h,
    wvu_h,
    wo_h,
    wg_h,
    wu_h,
    wd_h,
    out_result,
    out_latent,
    out_rope,
    table,
    cache,
    rope,
    wall,
    wkr,
    wku,
    wvu,
    wo,
    wgu,
    wd,
    xg,
    rows_all,
    gains,
    qsend,
    qrecv,
    qs,
    qt,
    nlat,
    nrope,
    hl,
    hsend,
    hrecv,
    asend,
    arecv,
    aq,
    srecv,
    mxsend,
    mxrecv,
    sl,
    xr,
    part,
    s1,
    xsend,
    xrecv,
    rsend,
    ret,
    msend,
    mrecv,
    nsend,
    nrecv,
    lines,
    folded,
    ku3,
    vu3,
    wide,
    sc,
    pb,
    w_sem,
    tp_send,
    tp_recv,
    p_send,
    p_recv,
    d_send,
    d_recv,
    x_send,
    x_recv,
    sib_send,
    sib_recv,
    s1_send,
    s1_recv,
    rx_send,
    rx_recv,
    ret_send,
    ret_recv,
    met,
):
    T, EP, R, LH, FT, REST, chunks, scale, places = cfg
    H = T * LH
    t = lax.axis_index("tp")
    e = lax.axis_index("ep")
    C = wku.shape[0]
    KD = wku.shape[1] // LH
    RD = wkr.shape[0]
    VD = wvu.shape[1] // LH
    D, WA = wall.shape
    F = wd.shape[0]
    LC = WA - LH * KD - LH * RD
    Q = D // T
    N = T * R
    RP = 2 * SUB
    QL = Q // LANES
    W = xr.shape[3]
    SPAN = cache.shape[1]
    HALF = R // 2
    HR = HALF * LH
    FOLD = D // 2
    pairs = T // 2
    sib = t + 1 - 2 * lax.rem(t, 2)

    def one_hot(i):
        row, n, m = places[i]
        return table[row : row + n, :m]

    def swap(k):
        other = e
        bit = 1
        while bit < EP:
            if k & bit:
                other = other + bit - 2 * bit * lax.rem(lax.div(e, bit), 2)
            bit *= 2
        return other

    loads = {}
    for i, (name, copies) in enumerate(
        [
            (
                "wall",
                [
                    (wq_h, wall.at[:, : LH * KD]),
                    (wqr_h, wall.at[:, LH * KD : LH * KD + LH * RD]),
                    (wl_h, wall.at[:, LH * KD + LH * RD :]),
                ],
            ),
            ("wkr", [(wkr_h, wkr)]),
            ("wku", [(wku_h, ku3)]),
            ("wvu", [(wvu_h, vu3)]),
            ("wo", [(wo_h, wo)]),
            ("wgu", [(wg_h.at[0], wgu.at[:, :F]), (wu_h.at[0], wgu.at[:, F:])]),
            ("wd", [(wd_h.at[0], wd)]),
            ("table", [(table_h, table)]),
            ("cache", [(cache_h.at[b], cache.at[b]) for b in range(R)]),
            ("rope", [(rope_h, rope)]),
        ]
    ):
        loads[name] = (i, copies)
    whole = {
        "wall": wall,
        "wkr": wkr,
        "wku": ku3,
        "wvu": vu3,
        "wo": wo,
        "wgu": wgu,
        "wd": wd,
        "table": table,
        "cache": cache,
        "rope": rope,
    }

    def fetch(name):
        i, copies = loads[name]
        for src, dst in copies:
            pltpu.make_async_copy(src, dst, w_sem.at[i]).start()

    def arrive(name):
        i, _ = loads[name]
        pltpu.make_async_copy(whole[name], whole[name], w_sem.at[i]).wait()

    for name in ("wku", "wkr", "wall", "table"):
        fetch(name)

    barrier = pltpu.get_barrier_semaphore()
    for k in range(1, T):
        pl.semaphore_signal(
            barrier, inc=1, device_id={"tp": lax.rem(t + k, T)}, device_id_type=MESH
        )
    bits = [1 << i for i in range(EP.bit_length() - 1)]

    def greet(sem):
        for k in bits:
            pl.semaphore_signal(sem, inc=1, device_id={"ep": swap(k)}, device_id_type=MESH)

    greet(barrier)

    def gain(ref):
        return ref[...].astype(F32)[None, :]

    def by_head_columns(source, target):
        size = source.shape[2]
        wide[...] = source[...].astype(F32).reshape(C * LH, size)
        for h in range(LH):
            target[:, h * size : (h + 1) * size] = wide[pl.ds(h, C, stride=LH), :].astype(BF16)

    def settle_recv(ref, sem):
        remote(ref, ref, sem, sem, {"tp": sib}).wait_recv()

    def settle_send(ref, sem):
        remote(ref, ref, sem, sem, {"tp": sib}).wait_send()

    def gather_tp(phase, src, dst):
        for k in range(1, T):
            peer = lax.rem(t + k, T)
            remote(
                src, dst.at[t], tp_send.at[phase], tp_recv.at[phase], {"tp": peer}
            ).start()

    def scatter_tp(phase, src, dst):
        for k in range(1, T):
            peer = lax.rem(t + k, T)
            remote(
                src.at[peer], dst.at[t], tp_send.at[phase], tp_recv.at[phase], {"tp": peer}
            ).start()
        dst[t] = src[t]

    sent_tp = []

    def finish_tp(phase, dst):
        settle_recv(dst.at[pl.ds(0, T - 1)], tp_recv.at[phase])
        sent_tp.append((phase, dst))

    token_values = jnp.concatenate(
        [tokens[...].astype(F32), jnp.zeros((RP - R, D), F32)], axis=0
    )
    left, right = token_values[SUB:, :FOLD], token_values[SUB:, FOLD:]
    xg[t] = jnp.concatenate(
        [token_values[:SUB], join_halves(left, right)], axis=1
    ).astype(BF16)
    pl.semaphore_wait(barrier, T - 1 + len(bits))

    gather_tp(0, xg.at[t], xg)
    fetch("cache")
    fetch("rope")
    greet(met.at[0])
    own_normed = rms_scale(token_values, gain(attn_gain)).astype(BF16)
    for i, ref in enumerate((post_attn_gain, ffn_gain)):
        gains[i : i + 1, :] = gain(ref)
    half = RD // 2
    lane = lax.broadcasted_iota(jnp.int32, (RP, RD), 1)
    row = lax.broadcasted_iota(jnp.int32, (RP, RD), 0)
    freqs = jnp.zeros((RP, RD), F32)
    for i in range(half):
        hit = (lane == i) | (lane == i + half)
        freqs = jnp.where(hit, np.float32(theta_base ** (-i / half)), freqs)
    positions = jnp.zeros((RP, RD), jnp.int32)
    for b in range(R):
        positions = jnp.where(row == b, lengths[b], positions)
    angles = positions.astype(F32) * freqs
    cosine = jnp.cos(angles)
    sine = jnp.sin(angles)
    sine = jnp.where(lane < half, -sine, sine)
    arrive("wku")
    by_head_columns(ku3, wku)
    arrive("wkr")
    key_raw = dot_nt(own_normed, wkr[...]).astype(BF16).astype(F32)
    new_rope = turn(key_raw, cosine, sine).astype(BF16)
    nrope[...] = new_rope.astype(F32)
    out_rope[...] = new_rope[:R]
    arrive("wall")
    arrive("table")
    finish_tp(0, xg)

    blocks = [xg[s, :, :D].astype(F32) for s in range(T)]
    for p in range(pairs):
        first = xg[2 * p, :, D:].astype(F32)
        second = xg[2 * p + 1, :, D:].astype(F32)
        blocks.append(
            jnp.concatenate([join_halves(first, second), join_ends(first, second)], axis=1)
        )
    rows = jnp.concatenate(blocks, axis=0)
    rows_all[...] = rows.astype(BF16)
    row_square = jnp.sum(rows * rows, axis=1, keepdims=True)
    normed = (rows * lax.rsqrt(row_square * (1.0 / D) + eps_norm) * gain(attn_gain)).astype(BF16)
    projected = dot(normed, wall[...])
    plain = projected[:, : LH * KD].astype(BF16)
    extra = projected[:, LH * KD :]
    lifted = [
        dot_nt(plain[:, h * KD : (h + 1) * KD], wku[:, h * KD : (h + 1) * KD])
        for h in range(LH)
    ]
    base = LH * C
    fold_base = base + (LH // 2) * C
    ROT = LH * RD
    for s in range(T):
        join = join_halves if s % 2 == 0 else join_ends
        top = slice(s * SUB, (s + 1) * SUB)
        rest = slice(T * SUB + (s // 2) * SUB, T * SUB + (s // 2 + 1) * SUB)
        for h in range(LH):
            qsend[s, :, h * C : (h + 1) * C] = lifted[h][top].astype(BF16)
        for h in range(0, LH, 2):
            at = base + (h // 2) * C
            qsend[s, :, at : at + C] = join(lifted[h][rest], lifted[h + 1][rest]).astype(BF16)
        at = fold_base
        qsend[s, :, at : at + ROT + LC] = extra[top].astype(BF16)
        at += ROT + LC
        tail = extra[rest]
        qsend[s, :, at : at + ROT // 2] = join(
            tail[:, : ROT // 2], tail[:, ROT // 2 : ROT]
        ).astype(BF16)
        at += ROT // 2
        tail_latent = tail[:, ROT:]
        qsend[s, :, at : at + LC] = join(tail_latent, tail_latent).astype(BF16)
    scatter_tp(1, qsend, qrecv)
    for name in ("wvu", "wo", "wgu", "wd"):
        fetch(name)
    for i in range(1, len(bits)):
        pl.semaphore_wait(met.at[i - 1], len(bits))
        if i < len(bits) - 1:
            greet(met.at[i])
    finish_tp(1, qrecv)

    at = fold_base
    latent_raw = jnp.concatenate(
        [
            jnp.concatenate(
                [
                    qrecv[s, :, at + ROT : at + ROT + LC],
                    qrecv[s, :, at + ROT + LC + ROT // 2 :],
                ],
                axis=0,
            )
            for s in range(T)
        ],
        axis=1,
    ).astype(F32)
    new_latent = rms_scale(latent_raw, gain(latent_gain)).astype(BF16)
    out_latent[...] = new_latent[:R]
    nlat[...] = new_latent.astype(F32)
    stacked = jnp.concatenate(
        [
            qrecv[s, :, i * C : (i + 1) * C]
            for s in range(T)
            for i in range(LH + LH // 2)
        ],
        axis=0,
    )
    qs[...] = dot(one_hot(0), stacked).astype(BF16).reshape(R, H, C)
    turned = []
    for s in range(T):
        head = qrecv[s, :, at : at + ROT].astype(F32)
        fold = qrecv[s, :, at + ROT + LC : at + ROT + LC + ROT // 2].astype(F32)
        tail = jnp.concatenate([fold, pltpu.roll(fold, SUB // 2, 0)], axis=1)
        rotary = jnp.concatenate([head, tail], axis=0)
        for h in range(LH):
            turned.append(turn(rotary[:, h * RD : (h + 1) * RD], cosine, sine).astype(BF16))
    qt[...] = dot(one_hot(1), jnp.concatenate(turned, axis=0)).astype(BF16).reshape(R, H, RD)

    arrive("cache")
    arrive("rope")
    position = lax.broadcasted_iota(jnp.int32, (H, SPAN), 1)
    for part_of in range(2):
        members = range(part_of * HALF, (part_of + 1) * HALF)
        for b in members:
            scores = (dot_nt(qs[b], cache[b]) + dot(qt[b], rope[b])) * scale
            sc[b] = jnp.where(position < lengths[b], scores, -jnp.inf)
        prob_own = {}
        for b in members:
            own = (
                jnp.sum(qs[b].astype(F32) * nlat[b : b + 1, :], axis=1, keepdims=True)
                + jnp.sum(qt[b].astype(F32) * nrope[b : b + 1, :], axis=1, keepdims=True)
            ) * scale
            masked = sc[b]
            highest = jnp.maximum(jnp.max(masked, axis=1, keepdims=True), own)
            raised = jnp.exp(masked - highest)
            raised_own = jnp.exp(own - highest)
            inverse = 1.0 / (jnp.sum(raised, axis=1, keepdims=True) + raised_own)
            pb[b] = (raised * inverse).astype(BF16)
            prob_own[b] = (raised_own * inverse).astype(BF16).astype(F32)
        for b in members:
            hl[b] = (dot(pb[b], cache[b]) + prob_own[b] * nlat[b : b + 1, :]).astype(BF16)
        attended = hl[part_of * HALF : (part_of + 1) * HALF].reshape(HALF * H, C)
        hsend[part_of] = dot(one_hot(2), attended).astype(BF16).reshape(T, HR, C)
        scatter_tp(2 + part_of, hsend.at[part_of], hrecv.at[part_of])

    lines[...] = jnp.zeros_like(lines)
    folded[...] = jnp.zeros_like(folded)
    arrive("wvu")
    by_head_columns(vu3, wvu)
    arrive("wo")
    group_of = one_hot(7).astype(F32).astype(jnp.int32) ^ e
    slot_of = one_hot(8).astype(F32)
    gi = lax.broadcasted_iota(jnp.int32, (N, N), 0)
    gj = lax.broadcasted_iota(jnp.int32, (N, N), 1)
    upper = (gi < gj).astype(F32).astype(BF16)
    lg = logits_t[...]
    lg = jnp.exp(lg - jnp.max(lg, axis=0, keepdims=True))
    weights = lg / jnp.sum(lg, axis=0, keepdims=True)
    count = jnp.zeros(slot_of.shape, F32)
    weighted = jnp.zeros(slot_of.shape, F32)
    for k in range(routes_t.shape[0]):
        hit = routes_t[k : k + 1, :] == group_of
        count = jnp.where(hit, 1.0, count)
        weighted = jnp.where(hit, weights[k : k + 1, :], weighted)
    rank = dot(count.astype(BF16), upper)
    taken = rank == slot_of
    weighted = jnp.where(taken, weighted, 0.0)
    weighted_hi = weighted.astype(BF16)
    weighted_lo = (weighted - weighted_hi.astype(F32)).astype(BF16)
    dispatch = dot_nt(jnp.where(taken, count, 0.0).astype(BF16), one_hot(4)).astype(BF16)
    spans, combines = [], []
    for lo, n in chunks:
        first = spans[-1][1] if spans else 0
        spans.append((first, first + n * (FT + REST) * SUB))
        span = slice(*spans[-1])
        combines.append(
            [dot_nt(one_hot(5), w[span]).astype(BF16) for w in (weighted_hi, weighted_lo)]
        )

    finish_tp(2, hrecv.at[0])
    finish_tp(3, hrecv.at[1])
    heads = dot(one_hot(3), hrecv[...].reshape(2 * T * HR, C)).astype(BF16)
    values = jnp.concatenate(
        [
            dot(heads[h * N : (h + 1) * N], wvu[:, h * VD : (h + 1) * VD]).astype(BF16)
            for h in range(LH)
        ],
        axis=1,
    )
    for q in range(T):
        asend[q] = dot(values, wo[:, q * Q : (q + 1) * Q]).astype(BF16)
    scatter_tp(4, asend, arecv)
    finish_tp(4, arecv)
    attn = arecv[0].astype(F32)
    for s in range(1, T):
        attn = attn + arecv[s].astype(F32)
    aq[t] = attn.astype(BF16)
    attn = attn.astype(BF16).astype(F32)

    def lanes_of(quarter):
        return pl.ds(pl.multiple_of(quarter * Q, Q), Q)

    def row_sum(v):
        return jnp.sum(v, axis=1, keepdims=True)

    def scaled_branch(attn, quarter):
        own_tokens = rows_all[:, lanes_of(quarter)].astype(F32)
        return own_tokens, attn * gains[0:1, lanes_of(quarter)]

    own_tokens, scaled = scaled_branch(attn, t)
    at_lane = lax.broadcasted_iota(jnp.int32, (N, LANES), 1)
    sums = jnp.where(at_lane == 0, row_sum(attn * attn), 0.0)
    sums = jnp.where(at_lane == 1, row_sum(own_tokens * scaled), sums)
    sums = jnp.where(at_lane == 2, row_sum(scaled * scaled), sums)
    sums = jnp.concatenate([sums, jnp.zeros((LANES - N, LANES), F32)], axis=0)
    srecv[t] = sums.T[:SUB]
    gather_tp(5, srecv.at[t], srecv)
    for j in range(1, pairs):
        remote(
            aq.at[t], aq.at[t], p_send.at[0], p_recv.at[j], {"tp": lax.rem(t + 2 * j, T)}
        ).start()
    finish_tp(5, srecv)
    totals = srecv[0]
    for s in range(1, T):
        totals = totals + srecv[s]
    totals = jnp.concatenate([totals, jnp.zeros((LANES - SUB, LANES), F32)], axis=0).T[:N]
    inverse = lax.rsqrt(totals[:, 0:1] * (1.0 / D) + eps_norm)
    square = row_square + 2.0 * inverse * totals[:, 1:2] + inverse * inverse * totals[:, 2:3]
    square = jnp.maximum(square, 0.0)
    ffn_inverse = lax.rsqrt(square * (1.0 / D) + eps_norm)

    def ffn_rows(own_tokens, scaled, quarter):
        mixed = (own_tokens + scaled * inverse).astype(BF16)
        normed = mixed.astype(F32) * ffn_inverse * gains[1:2, lanes_of(quarter)]
        return mixed, normed.astype(BF16)

    order = sorted(range(1, EP), key=lambda k: -k)
    far = EP // 2
    far_order, near_order = order[:far], order[far:]

    def quarter_at(j):
        return lax.rem(t + 2 * j, T)

    def pack_slots(j, c, normed):
        lo, n = chunks[c]
        picked = dot(dispatch[slice(*spans[c])], normed)
        for k in range(n):
            for i in range(FT):
                at = (k * FT + i) * SUB
                sl[j, lo + k, :, i * Q : (i + 1) * Q] = picked[at : at + SUB].astype(BF16)
        if REST:
            rest = picked[n * FT * SUB :]
            line = lax.broadcasted_iota(jnp.int32, (n * SUB, LANES), 0) & (SUB - 1)
            fold = jnp.zeros((n * SUB, LANES), F32)
            for i in range(QL):
                fold = jnp.where(line == i, rest[:, i * LANES : (i + 1) * LANES], fold)
            for k in range(n):
                sl[j, lo + k, :, FT * Q :] = fold[k * SUB : (k + 1) * SUB].astype(BF16)

    mixed, normed = ffn_rows(own_tokens, scaled, t)
    for c in range(1, len(chunks)):
        pack_slots(0, c, normed)
    for k in far_order:
        remote(sl.at[0, k], xr.at[t, k], d_send.at[0], d_recv.at[k], {"ep": swap(k)}).start()

    def send_near(j):
        for k in near_order:
            remote(
                sl.at[j, k], xr.at[quarter_at(j), k], d_send.at[1], d_recv.at[k], {"ep": swap(k)}
            ).start()
        xr[quarter_at(j), 0] = sl[j, 0]

    pack_slots(0, 0, normed)
    send_near(0)
    for j in range(1, pairs):
        settle_recv(aq.at[0], p_recv.at[pairs - j])
        other = quarter_at(j)
        _, normed = ffn_rows(*scaled_branch(aq[other].astype(F32), other), other)
        pack_slots(j, 0, normed)
        send_near(j)
    mxsend[...] = dot(one_hot(6), mixed).astype(BF16).reshape(T, RP, Q)
    scatter_tp(6, mxsend, mxrecv)

    chunk_of = {lo + k: c for c, (lo, n) in enumerate(chunks) for k in range(n)}
    far_chunks = range(1, len(chunks))

    def members(c):
        lo, n = chunks[c]
        return [k for k in order + [0] if lo <= k < lo + n]

    def to_sib(c, quarter, k):
        remote(
            xr.at[quarter, k], xr.at[quarter, k], sib_send.at[0], sib_recv.at[c], {"tp": sib}
        ).start()

    def relay_near(k):
        if k:
            settle_recv(xr.at[pl.ds(0, pairs), k], d_recv.at[k])
        for j in range(pairs):
            to_sib(0, quarter_at(j), k)

    relay_near(0)
    for k in far_order:
        settle_recv(xr.at[t, k], d_recv.at[k])
        for j in range(1, pairs):
            remote(
                xr.at[t, k], xr.at[t, k], x_send.at[0], x_recv.at[k, j], {"tp": quarter_at(j)}
            ).start()
        to_sib(chunk_of[k], t, k)
    for k in near_order[::-1]:
        relay_near(k)

    def relay_far(c):
        for k in members(c):
            for j in range(1, pairs):
                settle_recv(xr.at[t, k], x_recv.at[k, j])
                to_sib(c, lax.rem(t + T - 2 * j, T), k)

    def rows_of(blocks, c):
        return [
            blocks(k)[:, i * Q : (i + 1) * Q]
            for k in range(chunks[c][0], sum(chunks[c]))
            for i in range(FT)
        ]

    def folds_of(blocks, c):
        return [blocks(k)[:, FT * Q :] for k in range(chunks[c][0], sum(chunks[c]))]

    def experts(c):
        lo, n = chunks[c]
        settle_recv(xr.at[pl.ds(0, pairs), pl.ds(lo, n)], sib_recv.at[c])
        block = []
        folds = []
        for q in range(T):
            block.append(jnp.concatenate(rows_of(lambda k: xr.at[q, k], c), axis=0))
            if REST:
                for k in range(n):
                    fold = xr[q, lo + k, :, FT * Q :].astype(F32)
                    lines[c, q, pl.ds(k, QL, stride=SUB), :] = fold[:QL]
                folds += [lines[c, q, i * SUB : (i + 1) * SUB, :] for i in range(QL)]
        block = jnp.concatenate(block, axis=1)
        if REST:
            block = jnp.concatenate(
                [block, jnp.concatenate(folds, axis=1).astype(BF16)], axis=0
            )
        both = dot(block, wgu[...])
        gate = jnp.minimum(both[:, :F], clamp_limit)
        upward = jnp.clip(both[:, F:], -clamp_limit, clamp_limit)
        active = (upward + 1.0) * gate * (1.0 / (1.0 + jnp.exp(-sigmoid_alpha * gate)))
        active = active.astype(BF16)

        def down(quarter, step):
            cols = lanes_of(quarter)
            y = dot(active, wd[:, cols])
            for k in range(n):
                for i in range(FT):
                    at = (k * FT + i) * SUB
                    part[quarter, lo + k, :, i * Q : (i + 1) * Q] = y[at : at + SUB].astype(BF16)
            if REST:
                for i in range(QL):
                    folded[c, step, pl.ds(i, n, stride=SUB), :] = y[
                        n * FT * SUB : n * FT * SUB + n, i * LANES : (i + 1) * LANES
                    ]
                for k in range(n):
                    fold = folded[c, step, k * SUB : (k + 1) * SUB, :]
                    part[quarter, lo + k, :, FT * Q :] = fold.astype(BF16)

        for j in range(pairs - 1, -1, -1):
            quarter = lax.rem(sib + 2 * j, T)
            down(quarter, j)
            remote(
                part.at[quarter, pl.ds(lo, n)],
                s1.at[quarter, pl.ds(lo, n)],
                s1_send.at[0],
                s1_recv.at[c, j],
                {"tp": sib},
            ).start()
        for j in range(pairs - 1, -1, -1):
            down(quarter_at(j), pairs + j)

    def chip_sum(quarter, k):
        return part[quarter, k].astype(F32) + s1[quarter, k].astype(F32)

    def return_near():
        for j in range(pairs):
            settle_recv(s1.at[quarter_at(j), pl.ds(0, far)], s1_recv.at[0, j])
        for k in near_order:
            for j in range(pairs):
                rsend[j, k] = chip_sum(quarter_at(j), k).astype(BF16)
                remote(
                    rsend.at[j, k], ret.at[j, k], ret_send.at[1], ret_recv.at[1], {"ep": swap(k)}
                ).start()
        for j in range(pairs):
            ret[j, 0] = chip_sum(quarter_at(j), 0).astype(BF16)

    def reduce_far(c):
        lo, n = chunks[c]
        for j in range(pairs - 1, 0, -1):
            quarter = quarter_at(j)
            settle_recv(s1.at[quarter, pl.ds(lo, n)], s1_recv.at[c, j])
            for k in members(c):
                xsend[j, k] = chip_sum(quarter, k).astype(BF16)
                remote(
                    xsend.at[j, k], xrecv.at[j, k], rx_send.at[0], rx_recv.at[k, j], {"tp": quarter}
                ).start()

    def return_far(c):
        lo, n = chunks[c]
        settle_recv(s1.at[t, pl.ds(lo, n)], s1_recv.at[c, 0])
        for k in members(c):
            total = chip_sum(t, k)
            for j in range(1, pairs):
                settle_recv(xrecv.at[j, k], rx_recv.at[k, j])
                total = total + xrecv[j, k].astype(F32)
            rsend[0, k] = total.astype(BF16)
            remote(
                rsend.at[0, k], ret.at[0, k], ret_send.at[0], ret_recv.at[0], {"ep": swap(k)}
            ).start()

    def combine(j, c):
        rows = rows_of(lambda k: ret.at[j, k], c)
        if REST:
            n = chunks[c][1]
            fold = jnp.concatenate(folds_of(lambda k: ret.at[j, k], c), axis=0).astype(F32)
            line = lax.broadcasted_iota(jnp.int32, (n * SUB, LANES), 0) & (SUB - 1)
            lanes = [jnp.where(line == i, fold, 0.0).astype(BF16) for i in range(QL)]
            rows.append(jnp.concatenate(lanes, axis=1))
        rows = jnp.concatenate(rows, axis=0)
        return sum(dot(w, rows) for w in combines[c])

    arrive("wgu")
    arrive("wd")
    experts(0)
    relay_far(1)
    return_near()
    experts(1)
    reduce_far(1)
    return_far(1)
    settle_recv(ret.at[pl.ds(0, pairs), pl.ds(1, far - 1)], ret_recv.at[1])
    for j in range(pairs):
        nsend[:, j] = combine(j, 0).astype(BF16).reshape(T, RP, Q)
    scatter_tp(8, nsend, nrecv)
    settle_recv(ret.at[0, pl.ds(far, far)], ret_recv.at[0])
    far_part = sum(combine(0, c) for c in far_chunks)
    msend[...] = far_part.astype(BF16).reshape(T, RP, Q)
    scatter_tp(7, msend, mrecv)
    finish_tp(6, mxrecv)
    finish_tp(8, nrecv)
    finish_tp(7, mrecv)
    moe = []
    for q in range(T):
        total = mrecv[q].astype(F32)
        for j in range(pairs):
            total = total + nrecv[(q + T - 2 * j) % T, j].astype(F32)
        moe.append(total)
    moe = jnp.concatenate(moe, axis=1).astype(BF16).astype(F32)
    mixed_own = jnp.concatenate([mxrecv[s] for s in range(T)], axis=1).astype(F32)
    out_result[...] = (mixed_own + rms_scale(moe, gain(post_ffn_gain))).astype(BF16)[:R]

    for phase, dst in sent_tp:
        settle_send(dst.at[pl.ds(0, T - 1)], tp_send.at[phase])
    settle_send(xr.at[0, pl.ds(0, far)], d_send.at[0])
    settle_send(xr.at[pl.ds(0, pairs), pl.ds(1, far - 1)], d_send.at[1])
    if pairs > 1:
        settle_send(aq.at[pl.ds(0, pairs - 1)], p_send.at[0])
        settle_send(xr.at[pl.ds(0, pairs - 1), pl.ds(0, far)], x_send.at[0])
        settle_send(xsend.at[pl.ds(1, pairs - 1), pl.ds(0, far)], rx_send.at[0])
    settle_send(xr.at[pl.ds(0, pairs)], sib_send.at[0])
    settle_send(part.at[pl.ds(0, pairs)], s1_send.at[0])
    settle_send(xr.at[0, pl.ds(0, far)], ret_send.at[0])
    settle_send(xr.at[pl.ds(0, pairs), pl.ds(1, far - 1)], ret_send.at[1])


def hand_over(result, latent, rope, out_result, out_latent, out_rope):
    out_result[...] = result[...]
    out_latent[...] = latent[...]
    out_rope[...] = rope[...]


def body(
    tokens,
    cache_latent,
    cache_rope,
    lengths,
    attn_gain,
    latent_gain,
    post_attn_gain,
    ffn_gain,
    post_ffn_gain,
    w_query,
    w_query_rot,
    w_latent,
    w_key_rot,
    w_key_up,
    w_value_up,
    w_out,
    route_logits,
    routes,
    w_gate,
    w_up,
    w_down,
):
    R, D = tokens.shape
    T = lax.axis_size("tp")
    EP = lax.axis_size("ep")
    C, LH, KD = w_key_up.shape
    RD = w_key_rot.shape[1]
    VD = w_value_up.shape[2]
    H = T * LH
    K = routes.shape[1]
    scale = (KD + RD) ** (-0.5)
    RP = 2 * SUB
    assert R == SUB + SUB // 2 and T % 2 == 0 and LH % 2 == 0
    assert EP & (EP - 1) == 0 and T * R <= LANES
    cap = (R * T * K + EP - 1) // EP + 1
    Q = D // T
    F = w_gate.shape[2]
    LC = w_latent.shape[1]
    SPAN = cache_latent.shape[1]
    N = T * R
    QL = Q // LANES
    FT, REST = cap // SUB, cap % SUB
    if REST > 1 or QL > SUB:
        FT, REST = -(-cap // SUB), 0
    W = FT * Q + REST * LANES
    far = EP // 2
    chunks = ((0, far), (far, far))
    table, places = layout(T, R, LH, chunks, FT, REST, QL)

    vm = pl.BlockSpec(memory_space=pltpu.VMEM)
    hbm = pl.BlockSpec(memory_space=pl.ANY)
    dma = pltpu.SemaphoreType.DMA
    pairs = T // 2
    ROT = LH * RD
    QW = (LH + LH // 2) * C + ROT + LC + ROT // 2 + LC

    def v(*shape, dtype=BF16):
        return pltpu.VMEM(shape, dtype)

    cfg = (T, EP, R, LH, FT, REST, chunks, scale, places)
    outs = pl.pallas_call(
        functools.partial(kernel, cfg),
        out_shape=(
            jax.ShapeDtypeStruct((R, D), BF16),
            jax.ShapeDtypeStruct((R, C), BF16),
            jax.ShapeDtypeStruct((R, RD), BF16),
        ),
        in_specs=[pl.BlockSpec(memory_space=pltpu.SMEM)] + [vm] * 8 + [hbm] * 13,
        out_specs=(vm, vm, vm),
        scratch_shapes=[
            v(*table.shape),
            v(R, SPAN, C),
            v(R, RD, SPAN),
            v(D, LH * KD + ROT + LC),
            v(RD, D),
            v(C, LH * KD),
            v(C, LH * VD),
            v(LH * VD, D),
            v(D, 2 * F),
            v(F, D),
            v(T, SUB, D + D // 2),
            v(N, D),
            v(SUB, D, dtype=F32),
            v(T, SUB, QW),
            v(T, SUB, QW),
            v(R, H, C),
            v(R, H, RD),
            v(RP, C, dtype=F32),
            v(RP, RD, dtype=F32),
            v(R, H, C),
            v(2, T, R // 2 * LH, C),
            v(2, T, R // 2 * LH, C),
            v(T, N, Q),
            v(T, N, Q),
            v(T, N, Q),
            v(T, SUB, LANES, dtype=F32),
            v(T, RP, Q),
            v(T, RP, Q),
            v(pairs, EP, SUB, W),
            v(T, EP, SUB, W),
            v(T, EP, SUB, W),
            v(T, EP, SUB, W),
            v(pairs, EP, SUB, W),
            v(pairs, EP, SUB, W),
            v(pairs, EP, SUB, W),
            v(pairs, EP, SUB, W),
            v(T, RP, Q),
            v(T, RP, Q),
            v(T, pairs, RP, Q),
            v(T, pairs, RP, Q),
            v(len(chunks), T, QL * SUB, LANES, dtype=F32),
            v(len(chunks), T, far * SUB, LANES, dtype=F32),
            v(C, LH, KD),
            v(C, LH, VD),
            v(C * LH, KD, dtype=F32),
            v(R, H, SPAN, dtype=F32),
            v(R, H, SPAN),
            dma((10,)),
            dma((9,)),
            dma((9,)),
            dma((1,)),
            dma((pairs,)),
            dma((2,)),
            dma((EP,)),
            dma((1,)),
            dma((EP, pairs)),
            dma((1,)),
            dma((len(chunks),)),
            dma((1,)),
            dma((len(chunks), pairs)),
            dma((1,)),
            dma((EP, pairs)),
            dma((2,)),
            dma((2,)),
            pltpu.SemaphoreType.REGULAR((max(1, EP.bit_length() - 2),)),
        ],
        compiler_params=pltpu.CompilerParams(
            collective_id=0, has_side_effects=True, vmem_limit_bytes=60 * 1024 * 1024
        ),
    )(
        lengths,
        tokens,
        attn_gain,
        latent_gain,
        post_attn_gain,
        ffn_gain,
        post_ffn_gain,
        routes.T,
        route_logits.T,
        jnp.asarray(table, BF16),
        cache_latent,
        cache_rope,
        w_query,
        w_query_rot,
        w_latent,
        w_key_rot.T,
        w_key_up,
        w_value_up,
        w_out,
        w_gate,
        w_up,
        w_down,
    )
    return pl.pallas_call(
        hand_over,
        out_shape=tuple(jax.ShapeDtypeStruct(o.shape, o.dtype) for o in outs),
        in_specs=[vm] * 3,
        out_specs=(vm, vm, vm),
    )(*outs)


def solution(mesh):
    return jax.shard_map(
        body,
        mesh=mesh,
        in_specs=(
            P(("ep", "tp"), None),
            P(("ep", "tp"), None, None),
            P(("ep", "tp"), None, None),
            P(("ep", "tp")),
            P(),
            P(),
            P(),
            P(),
            P(),
            P(None, "tp"),
            P(None, "tp"),
            P(None, "tp"),
            P(),
            P(None, "tp", None),
            P(None, "tp", None),
            P("tp", None),
            P("ep", None),
            P("ep", None),
            P("ep", None, "tp"),
            P("ep", None, "tp"),
            P("ep", "tp", None),
        ),
        out_specs=(P(("ep", "tp"), None), P(("ep", "tp"), None), P(("ep", "tp"), None)),
        check_vma=False,
    )
```

```python
import functools

import jax
import jax.numpy as jnp
import numpy as np
from jax import lax
from jax.experimental import pallas as pl
from jax.experimental.pallas import tpu as pltpu
from jax.sharding import PartitionSpec as P

eps_norm = 1e-06
clamp_limit = 7.0
sigmoid_alpha = 1.702
theta_base = 10000.0
MESH = pl.DeviceIdType.MESH
F32 = jnp.float32
BF16 = jnp.bfloat16
SUB = 8
LANES = 128


def rms_scale(values, gain):
    mean_square = jnp.mean(values * values, axis=-1, keepdims=True)
    return values * lax.rsqrt(mean_square + eps_norm) * gain


def turn(values, cosine, sine):
    half = values.shape[-1] // 2
    swapped = jnp.concatenate([values[:, half:], values[:, :half]], axis=1)
    return values * cosine + swapped * sine


def dot(a, b):
    return jnp.dot(a, b, preferred_element_type=F32)


def dot_nt(a, b):
    return lax.dot_general(a, b, (((1,), (1,)), ((), ())), preferred_element_type=F32)


def remote(src, dst, send_sem, recv_sem, where):
    return pltpu.make_async_remote_copy(
        src_ref=src,
        dst_ref=dst,
        send_sem=send_sem,
        recv_sem=recv_sem,
        device_id=where,
        device_id_type=MESH,
    )


def half_rows(values):
    return lax.broadcasted_iota(jnp.int32, values.shape, 0) < SUB // 2


def join_halves(upper, lower):
    return jnp.where(half_rows(upper), upper, pltpu.roll(lower, SUB // 2, 0))


def join_ends(upper, lower):
    return jnp.where(half_rows(upper), pltpu.roll(upper, SUB // 2, 0), lower)


def layout(T, R, LH, chunks, FT, REST, QL):
    H = T * LH
    tail = R - SUB
    mid = LH // 2

    def packed(s, b):
        if b < SUB:
            return s * SUB + b
        return T * SUB + (s // 2) * SUB + (s % 2) * tail + b - SUB

    to_seq = np.zeros((SUB * H, H * SUB))
    to_seq_tail = np.zeros((tail * H, T * mid * SUB))
    to_turn_tail = np.zeros((tail * H, T * mid * SUB))
    to_head = np.zeros((H * SUB, SUB * H))
    to_head_tail = np.zeros((H * tail, tail * H))
    to_value = np.zeros((LH * T * R, LH * T * R))
    for s in range(T):
        for h in range(LH):
            head = s * LH + h
            for b in range(SUB):
                to_seq[b * H + head, head * SUB + b] = 1
                to_head[head * SUB + b, b * H + head] = 1
                to_value[h * T * R + packed(s, b), head * SUB + b] = 1
            for b in range(tail):
                at = (s * mid + h // 2) * SUB + (h % 2) * tail + b
                to_seq_tail[b * H + head, at] = 1
                at = (s * mid + h % mid) * SUB + (h // mid) * tail + b
                to_turn_tail[b * H + head, at] = 1
                to_head_tail[head * tail + b, b * H + head] = 1
                at = H * SUB + head * tail + b
                to_value[h * T * R + packed(s, SUB + b), at] = 1
    spread = np.zeros((T * R, T * R))
    own_natural = np.zeros((T * 2 * SUB, T * R))
    own_packed = np.zeros((T * 2 * SUB, T * R))
    for s in range(T):
        for b in range(R):
            spread[packed(s, b), s * R + b] = 1
            own_natural[s * 2 * SUB + b, s * R + b] = 1
            own_packed[s * 2 * SUB + b, packed(s, b)] = 1
    groups, slots = [], []
    for lo, n in chunks:
        for k in range(n):
            groups += [lo + k] * (FT * SUB)
            slots += range(FT * SUB)
        for k in range(n if REST else 0):
            groups += [lo + k] * SUB
            slots += [FT * SUB] * QL + [-1] * (SUB - QL)
    group_of = np.repeat(np.array(groups)[:, None], T * R, 1)
    slot_of = np.repeat(np.array(slots)[:, None], T * R, 1)
    parts = [to_seq, to_seq_tail, to_turn_tail, to_value, spread, own_natural, own_packed]
    parts += [group_of, slot_of, to_head, to_head_tail]
    width = max(p.shape[1] for p in parts)
    rows, places = 0, []
    for p in parts:
        places.append((rows, p.shape[0], p.shape[1]))
        rows += -(-p.shape[0] // 16) * 16
    table = np.zeros((rows, width), np.float32)
    for p, (row, n, m) in zip(parts, places):
        table[row : row + n, :m] = p
    return table, tuple(places)


def kernel(
    cfg,
    lengths_h,
    tokens_h,
    attn_gain_h,
    latent_gain_h,
    post_attn_gain_h,
    ffn_gain_h,
    post_ffn_gain_h,
    routes_t_h,
    logits_t_h,
    table_h,
    cache_h,
    rope_h,
    wq_h,
    wqr_h,
    wl_h,
    wkr_h,
    wku_h,
    wvu_h,
    wo_h,
    wg_h,
    wu_h,
    wd_h,
    out_result_h,
    out_latent_h,
    out_rope_h,
    lengths,
    tokens,
    attn_gain,
    latent_gain,
    post_attn_gain,
    ffn_gain,
    post_ffn_gain,
    routes_t,
    logits_t,
    out_result,
    out_latent,
    out_rope,
    table,
    cache,
    rope,
    wall,
    wkr,
    wku,
    wvu,
    wo,
    wgu,
    wd,
    xg,
    rows_all,
    gains,
    qsend,
    qrecv,
    qs,
    qt,
    nlat,
    nrope,
    hl,
    hsend,
    hrecv,
    hsend_tail,
    hrecv_tail,
    asend,
    arecv,
    aq,
    srecv,
    mxsend,
    mxrecv,
    sl,
    xr,
    part,
    s1,
    xsend,
    xrecv,
    rsend,
    ret,
    msend,
    mrecv,
    nsend,
    nrecv,
    lines,
    folded,
    ku3,
    vu3,
    wide,
    sc,
    pb,
    w_sem,
    tp_send,
    tp_recv,
    p_send,
    p_recv,
    d_send,
    d_recv,
    x_send,
    x_recv,
    sib_send,
    sib_recv,
    s1_send,
    s1_recv,
    rx_send,
    rx_recv,
    ret_send,
    ret_recv,
    met,
):
    T, EP, R, LH, FT, REST, chunks, scale, places = cfg
    H = T * LH
    t = lax.axis_index("tp")
    e = lax.axis_index("ep")
    C = wku.shape[0]
    KD = wku.shape[1] // LH
    RD = wkr.shape[0]
    VD = wvu.shape[1] // LH
    D, WA = wall.shape
    F = wd.shape[0]
    LC = WA - LH * KD - LH * RD
    Q = D // T
    N = T * R
    RP = 2 * SUB
    QL = Q // LANES
    W = xr.shape[3]
    SPAN = cache.shape[1]
    tail = R - SUB
    mid = LH // 2
    FOLD = D // 2
    pairs = T // 2
    sib = t + 1 - 2 * lax.rem(t, 2)

    def one_hot(i):
        row, n, m = places[i]
        return table[row : row + n, :m]

    def swap(k):
        other = e
        bit = 1
        while bit < EP:
            if k & bit:
                other = other + bit - 2 * bit * lax.rem(lax.div(e, bit), 2)
            bit *= 2
        return other

    loads = {}
    for i, (name, copies) in enumerate(
        [
            (
                "wall",
                [
                    (wq_h, wall.at[:, : LH * KD]),
                    (wqr_h, wall.at[:, LH * KD : LH * KD + LH * RD]),
                    (wl_h, wall.at[:, LH * KD + LH * RD :]),
                ],
            ),
            ("wkr", [(wkr_h, wkr)]),
            ("wku", [(wku_h, ku3)]),
            ("wvu", [(wvu_h, vu3)]),
            ("wo", [(wo_h, wo)]),
            ("wgu", [(wg_h.at[0], wgu.at[:, :F]), (wu_h.at[0], wgu.at[:, F:])]),
            ("wd", [(wd_h.at[0], wd)]),
            ("table", [(table_h, table)]),
            ("cache", [(cache_h.at[b], cache.at[b]) for b in range(R)]),
            ("rope", [(rope_h, rope)]),
            ("tokens", [(tokens_h, tokens)]),
            ("lengths", [(lengths_h, lengths)]),
            ("attn_gain", [(attn_gain_h, attn_gain)]),
            ("latent_gain", [(latent_gain_h, latent_gain)]),
            ("post_attn_gain", [(post_attn_gain_h, post_attn_gain)]),
            ("ffn_gain", [(ffn_gain_h, ffn_gain)]),
            ("post_ffn_gain", [(post_ffn_gain_h, post_ffn_gain)]),
            ("routes", [(routes_t_h, routes_t)]),
            ("logits", [(logits_t_h, logits_t)]),
        ]
    ):
        loads[name] = (i, copies)
    for name, copies in (
        ("out_rope", (out_rope, out_rope_h)),
        ("out_latent", (out_latent, out_latent_h)),
        ("out_result", (out_result, out_result_h)),
    ):
        earlier = {"out_rope": "tokens", "out_latent": "wall", "out_result": "wkr"}[name]
        loads[name] = (loads[earlier][0], [copies])
    whole = {"wall": wall, "wgu": wgu, "cache": cache}

    def fetch(name):
        i, copies = loads[name]
        for src, dst in copies:
            pltpu.make_async_copy(src, dst, w_sem.at[i]).start()

    def arrive(name):
        i, copies = loads[name]
        src, dst = (whole[name], whole[name]) if name in whole else copies[0]
        pltpu.make_async_copy(src, dst, w_sem.at[i]).wait()

    fetch("tokens")
    barrier = pltpu.get_barrier_semaphore()
    for k in range(1, T):
        pl.semaphore_signal(
            barrier, inc=1, device_id={"tp": lax.rem(t + k, T)}, device_id_type=MESH
        )
    bits = [1 << i for i in range(EP.bit_length() - 1)]

    def greet(sem):
        for k in bits:
            pl.semaphore_signal(sem, inc=1, device_id={"ep": swap(k)}, device_id_type=MESH)

    greet(barrier)
    for name in ("attn_gain", "lengths", "post_attn_gain", "ffn_gain", "latent_gain"):
        fetch(name)
    for name in ("wku", "wkr", "wall", "table", "post_ffn_gain", "routes", "logits"):
        fetch(name)

    def gain(ref):
        return ref[...].astype(F32)[None, :]

    def by_head_columns(source, target):
        size = source.shape[2]
        wide[...] = source[...].astype(F32).reshape(C * LH, size)
        for h in range(LH):
            target[:, h * size : (h + 1) * size] = wide[pl.ds(h, C, stride=LH), :].astype(BF16)

    def settle_recv(ref, sem):
        remote(ref, ref, sem, sem, {"tp": sib}).wait_recv()

    def settle_send(ref, sem):
        remote(ref, ref, sem, sem, {"tp": sib}).wait_send()

    sent_tp = {}
    send_of = {0: 0, 1: 1, 9: 2, 2: 0, 3: 1, 4: 2, 5: 0, 6: 1, 8: 2, 7: 0}

    def reuse_send(phase):
        slot = send_of[phase]
        if slot in sent_tp:
            settle_send(sent_tp.pop(slot), tp_send.at[slot])
        return tp_send.at[slot]

    peers = [lax.rem(c + 2 * j, T) for c in (t, sib) for j in range(1, pairs)] + [sib]

    def gather_tp(phase, src, dst):
        sent = reuse_send(phase)
        for peer in peers:
            remote(
                src, dst.at[t], sent, tp_recv.at[phase], {"tp": peer}
            ).start()

    def scatter_tp(phase, src, dst):
        sent = reuse_send(phase)
        for peer in peers:
            remote(
                src.at[peer], dst.at[t], sent, tp_recv.at[phase], {"tp": peer}
            ).start()
        dst[t] = src[t]


    def finish_tp(phase, dst, lanes=None):
        view = dst.at[pl.ds(0, T - 1)] if lanes is None else dst.at[pl.ds(0, T - 1), :, lanes]
        settle_recv(view, tp_recv.at[phase])
        sent_tp[send_of[phase]] = view

    arrive("tokens")
    token_values = jnp.concatenate(
        [tokens[...].astype(F32), jnp.zeros((RP - R, D), F32)], axis=0
    )
    left, right = token_values[SUB:, :FOLD], token_values[SUB:, FOLD:]
    xg[t] = jnp.concatenate(
        [token_values[:SUB], join_halves(left, right)], axis=1
    ).astype(BF16)
    pl.semaphore_wait(barrier, T - 1 + len(bits))

    gather_tp(0, xg.at[t], xg)
    fetch("cache")
    fetch("rope")
    greet(met.at[0])
    for name in ("attn_gain", "lengths", "post_attn_gain", "ffn_gain"):
        arrive(name)
    own_normed = rms_scale(token_values, gain(attn_gain)).astype(BF16)
    for i, ref in enumerate((post_attn_gain, ffn_gain)):
        gains[i : i + 1, :] = gain(ref)
    half = RD // 2
    lane = lax.broadcasted_iota(jnp.int32, (RP, RD), 1)
    row = lax.broadcasted_iota(jnp.int32, (RP, RD), 0)
    freqs = jnp.zeros((RP, RD), F32)
    for i in range(half):
        hit = (lane == i) | (lane == i + half)
        freqs = jnp.where(hit, np.float32(theta_base ** (-i / half)), freqs)
    positions = jnp.zeros((RP, RD), jnp.int32)
    for b in range(R):
        positions = jnp.where(row == b, lengths[b], positions)
    angles = positions.astype(F32) * freqs
    cosine = jnp.cos(angles)
    sine = jnp.sin(angles)
    sine = jnp.where(lane < half, -sine, sine)
    arrive("wku")
    by_head_columns(ku3, wku)
    arrive("wkr")
    key_raw = dot_nt(own_normed, wkr[...]).astype(BF16).astype(F32)
    new_rope = turn(key_raw, cosine, sine).astype(BF16)
    nrope[...] = new_rope.astype(F32)
    out_rope[...] = new_rope[:R]
    fetch("out_rope")
    arrive("wall")
    arrive("table")
    finish_tp(0, xg)

    blocks = [xg[s, :, :D].astype(F32) for s in range(T)]
    for p in range(pairs):
        first = xg[2 * p, :, D:].astype(F32)
        second = xg[2 * p + 1, :, D:].astype(F32)
        blocks.append(
            jnp.concatenate([join_halves(first, second), join_ends(first, second)], axis=1)
        )
    rows = jnp.concatenate(blocks, axis=0)
    rows_all[...] = rows.astype(BF16)
    row_square = jnp.sum(rows * rows, axis=1, keepdims=True)
    normed = (rows * lax.rsqrt(row_square * (1.0 / D) + eps_norm) * gain(attn_gain)).astype(BF16)
    projected = dot(normed, wall[...])
    plain = projected[:, : LH * KD].astype(BF16)
    extra = projected[:, LH * KD :]
    lifted = [
        dot_nt(plain[:, h * KD : (h + 1) * KD], wku[:, h * KD : (h + 1) * KD])
        for h in range(LH)
    ]
    ROT = LH * RD
    split = LH * C + ROT + LC
    turn_tail = split + mid * C
    early, late = pl.ds(0, split), pl.ds(split, qsend.shape[2] - split)

    def send_queries(phase, lanes):
        sent = reuse_send(phase)
        for peer in peers:
            remote(
                qsend.at[peer, :, lanes],
                qrecv.at[t, :, lanes],
                sent,
                tp_recv.at[phase],
                {"tp": peer},
            ).start()

    for s in range(T):
        top = slice(s * SUB, (s + 1) * SUB)
        for h in range(LH):
            qsend[s, :, h * C : (h + 1) * C] = lifted[h][top].astype(BF16)
        qsend[s, :, LH * C : split] = extra[top].astype(BF16)
    send_queries(1, early)
    for s in range(T):
        join = join_halves if s % 2 == 0 else join_ends
        rest = slice(T * SUB + (s // 2) * SUB, T * SUB + (s // 2 + 1) * SUB)
        for h in range(0, LH, 2):
            at = split + (h // 2) * C
            qsend[s, :, at : at + C] = join(lifted[h][rest], lifted[h + 1][rest]).astype(BF16)
        last = extra[rest]
        at = turn_tail
        qsend[s, :, at : at + ROT // 2] = join(
            last[:, : ROT // 2], last[:, ROT // 2 : ROT]
        ).astype(BF16)
        at += ROT // 2
        last = last[:, ROT:]
        qsend[s, :, at : at + LC] = join(last, last).astype(BF16)
    send_queries(9, late)
    qrecv[t] = qsend[t]
    for name in ("wvu", "wo", "wgu", "wd"):
        fetch(name)
    for i in range(1, len(bits)):
        pl.semaphore_wait(met.at[i - 1], len(bits))
        if i < len(bits) - 1:
            greet(met.at[i])
    finish_tp(1, qrecv, early)

    arrive("latent_gain")

    def fresh_latent(at):
        raw = jnp.concatenate([qrecv[s, :, at : at + LC] for s in range(T)], axis=1)
        return rms_scale(raw.astype(F32), gain(latent_gain)).astype(BF16)

    def queries(first, table_of, blocks):
        stacked = jnp.concatenate(blocks, axis=0)
        rows = dot(table_of, stacked).astype(BF16)
        return rows.reshape(first, H, stacked.shape[1])

    def turned(at, count, cosine, sine):
        return [
            turn(qrecv[s, :, at + i * RD : at + (i + 1) * RD].astype(F32), cosine, sine).astype(BF16)
            for s in range(T)
            for i in range(count)
        ]

    def blocks_of(at, count):
        return [qrecv[s, :, at + i * C : at + (i + 1) * C] for s in range(T) for i in range(count)]

    latent = fresh_latent(LH * C + ROT)
    out_latent[:SUB] = latent
    nlat[:SUB] = latent.astype(F32)
    qs[:SUB] = queries(SUB, one_hot(0), blocks_of(0, LH))
    qt[:SUB] = queries(SUB, one_hot(0), turned(LH * C, LH, cosine[:SUB], sine[:SUB]))

    def late_queries():
        finish_tp(9, qrecv, late)
        latent = fresh_latent(turn_tail + ROT // 2)
        out_latent[SUB:] = latent[:tail]
        fetch("out_latent")
        nlat[SUB:] = latent.astype(F32)
        qs[SUB:] = queries(tail, one_hot(1), blocks_of(split, mid))
        cos, sin = cosine[SUB:], sine[SUB:]
        cos, sin = join_halves(cos, cos), join_halves(sin, sin)
        qt[SUB:] = queries(tail, one_hot(2), turned(turn_tail, mid, cos, sin))

    arrive("cache")
    arrive("rope")
    position = lax.broadcasted_iota(jnp.int32, (H, SPAN), 1)
    for members, table_of, phase, send, recv in (
        (range(SUB), one_hot(9), 2, hsend, hrecv),
        (range(SUB, R), one_hot(10), 3, hsend_tail, hrecv_tail),
    ):
        if phase == 3:
            late_queries()
        for b in members:
            scores = (dot_nt(qs[b], cache[b]) + dot(qt[b], rope[b])) * scale
            sc[b] = jnp.where(position < lengths[b], scores, -jnp.inf)
        prob_own = {}
        for b in members:
            own = (
                jnp.sum(qs[b].astype(F32) * nlat[b : b + 1, :], axis=1, keepdims=True)
                + jnp.sum(qt[b].astype(F32) * nrope[b : b + 1, :], axis=1, keepdims=True)
            ) * scale
            masked = sc[b]
            highest = jnp.maximum(jnp.max(masked, axis=1, keepdims=True), own)
            raised = jnp.exp(masked - highest)
            raised_own = jnp.exp(own - highest)
            inverse = 1.0 / (jnp.sum(raised, axis=1, keepdims=True) + raised_own)
            pb[b] = (raised * inverse).astype(BF16)
            prob_own[b] = (raised_own * inverse).astype(BF16).astype(F32)
        for b in members:
            hl[b] = (dot(pb[b], cache[b]) + prob_own[b] * nlat[b : b + 1, :]).astype(BF16)
        count = len(members)
        attended = hl[members[0] : members[0] + count].reshape(count * H, C)
        send[...] = dot(table_of, attended).astype(BF16).reshape(T, count * LH, C)
        scatter_tp(phase, send, recv)

    lines[...] = jnp.zeros_like(lines)
    folded[...] = jnp.zeros_like(folded)
    for name in ("routes", "logits", "post_ffn_gain", "wvu"):
        arrive(name)
    by_head_columns(vu3, wvu)
    arrive("wo")
    group_of = one_hot(7).astype(F32).astype(jnp.int32) ^ e
    slot_of = one_hot(8).astype(F32)
    gi = lax.broadcasted_iota(jnp.int32, (N, N), 0)
    gj = lax.broadcasted_iota(jnp.int32, (N, N), 1)
    upper = (gi < gj).astype(F32).astype(BF16)
    lg = logits_t[...]
    lg = jnp.exp(lg - jnp.max(lg, axis=0, keepdims=True))
    weights = lg / jnp.sum(lg, axis=0, keepdims=True)
    count = jnp.zeros(slot_of.shape, F32)
    weighted = jnp.zeros(slot_of.shape, F32)
    for k in range(routes_t.shape[0]):
        hit = routes_t[k : k + 1, :] == group_of
        count = jnp.where(hit, 1.0, count)
        weighted = jnp.where(hit, weights[k : k + 1, :], weighted)
    rank = dot(count.astype(BF16), upper)
    taken = rank == slot_of
    weighted = jnp.where(taken, weighted, 0.0)
    weighted_hi = weighted.astype(BF16)
    weighted_lo = (weighted - weighted_hi.astype(F32)).astype(BF16)
    dispatch = dot_nt(jnp.where(taken, count, 0.0).astype(BF16), one_hot(4)).astype(BF16)
    spans, combines = [], []
    for lo, n in chunks:
        first = spans[-1][1] if spans else 0
        spans.append((first, first + n * (FT + REST) * SUB))
        span = slice(*spans[-1])
        combines.append(
            [dot_nt(one_hot(5), w[span]).astype(BF16) for w in (weighted_hi, weighted_lo)]
        )

    finish_tp(2, hrecv)
    finish_tp(3, hrecv_tail)
    attended = jnp.concatenate(
        [hrecv[...].reshape(H * SUB, C), hrecv_tail[...].reshape(H * tail, C)], axis=0
    )
    heads = dot(one_hot(3), attended).astype(BF16)
    values = jnp.concatenate(
        [
            dot(heads[h * N : (h + 1) * N], wvu[:, h * VD : (h + 1) * VD]).astype(BF16)
            for h in range(LH)
        ],
        axis=1,
    )

    def lanes_of(quarter):
        return pl.ds(pl.multiple_of(quarter * Q, Q), Q)

    sent = reuse_send(4)
    for peer in peers:
        asend[peer] = dot(values, wo[:, lanes_of(peer)]).astype(BF16)
        remote(
            asend.at[peer], arecv.at[t], sent, tp_recv.at[4], {"tp": peer}
        ).start()
    arecv[t] = dot(values, wo[:, lanes_of(t)]).astype(BF16)
    finish_tp(4, arecv)
    attn = arecv[0].astype(F32)
    for s in range(1, T):
        attn = attn + arecv[s].astype(F32)
    aq[t] = attn.astype(BF16)
    attn = attn.astype(BF16).astype(F32)

    def row_sum(v):
        return jnp.sum(v, axis=1, keepdims=True)

    def scaled_branch(attn, quarter):
        own_tokens = rows_all[:, lanes_of(quarter)].astype(F32)
        return own_tokens, attn * gains[0:1, lanes_of(quarter)]

    own_tokens, scaled = scaled_branch(attn, t)
    at_lane = lax.broadcasted_iota(jnp.int32, (N, LANES), 1)
    sums = jnp.where(at_lane == 0, row_sum(attn * attn), 0.0)
    sums = jnp.where(at_lane == 1, row_sum(own_tokens * scaled), sums)
    sums = jnp.where(at_lane == 2, row_sum(scaled * scaled), sums)
    sums = jnp.concatenate([sums, jnp.zeros((LANES - N, LANES), F32)], axis=0)
    srecv[t] = sums.T[:SUB]
    gather_tp(5, srecv.at[t], srecv)
    for j in range(1, pairs):
        remote(
            aq.at[t], aq.at[t], p_send.at[0], p_recv.at[j], {"tp": lax.rem(t + 2 * j, T)}
        ).start()
    finish_tp(5, srecv)
    totals = srecv[0]
    for s in range(1, T):
        totals = totals + srecv[s]
    totals = jnp.concatenate([totals, jnp.zeros((LANES - SUB, LANES), F32)], axis=0).T[:N]
    inverse = lax.rsqrt(totals[:, 0:1] * (1.0 / D) + eps_norm)
    square = row_square + 2.0 * inverse * totals[:, 1:2] + inverse * inverse * totals[:, 2:3]
    square = jnp.maximum(square, 0.0)
    ffn_inverse = lax.rsqrt(square * (1.0 / D) + eps_norm)

    def ffn_rows(own_tokens, scaled, quarter):
        mixed = (own_tokens + scaled * inverse).astype(BF16)
        normed = mixed.astype(F32) * ffn_inverse * gains[1:2, lanes_of(quarter)]
        return mixed, normed.astype(BF16)

    order = sorted(range(1, EP), key=lambda k: (-k.bit_length(), k ^ 1, k))
    far = EP // 2
    far_order, near_order = order[:far], order[far:]

    def quarter_at(j):
        return lax.rem(t + 2 * j, T)

    def pack_slots(j, c, normed):
        lo, n = chunks[c]
        picked = dot(dispatch[slice(*spans[c])], normed)
        for k in range(n):
            for i in range(FT):
                at = (k * FT + i) * SUB
                sl[j, lo + k, :, i * Q : (i + 1) * Q] = picked[at : at + SUB].astype(BF16)
        if REST:
            rest = picked[n * FT * SUB :]
            line = lax.broadcasted_iota(jnp.int32, (n * SUB, LANES), 0) & (SUB - 1)
            fold = jnp.zeros((n * SUB, LANES), F32)
            for i in range(QL):
                fold = jnp.where(line == i, rest[:, i * LANES : (i + 1) * LANES], fold)
            for k in range(n):
                sl[j, lo + k, :, FT * Q :] = fold[k * SUB : (k + 1) * SUB].astype(BF16)

    mixed, normed = ffn_rows(own_tokens, scaled, t)
    for c in range(1, len(chunks)):
        pack_slots(0, c, normed)
    for k in far_order:
        remote(sl.at[0, k], xr.at[t, k], d_send.at[0], d_recv.at[k], {"ep": swap(k)}).start()

    def send_near(j):
        for k in near_order:
            remote(
                sl.at[j, k], xr.at[quarter_at(j), k], d_send.at[1], d_recv.at[k], {"ep": swap(k)}
            ).start()
        xr[quarter_at(j), 0] = sl[j, 0]

    pack_slots(0, 0, normed)
    send_near(0)
    for j in range(1, pairs):
        settle_recv(aq.at[0], p_recv.at[pairs - j])
        other = quarter_at(j)
        _, normed = ffn_rows(*scaled_branch(aq[other].astype(F32), other), other)
        pack_slots(j, 0, normed)
        send_near(j)
    mxsend[...] = dot(one_hot(6), mixed).astype(BF16).reshape(T, RP, Q)
    scatter_tp(6, mxsend, mxrecv)

    chunk_of = {lo + k: c for c, (lo, n) in enumerate(chunks) for k in range(n)}
    far_chunks = range(1, len(chunks))

    def members(c):
        lo, n = chunks[c]
        return [k for k in order + [0] if lo <= k < lo + n]

    def to_sib(c, quarter, k):
        remote(
            xr.at[quarter, k], xr.at[quarter, k], sib_send.at[0], sib_recv.at[c], {"tp": sib}
        ).start()

    def relay_near(k):
        if k:
            settle_recv(xr.at[pl.ds(0, pairs), k], d_recv.at[k])
        for j in range(pairs):
            to_sib(0, quarter_at(j), k)

    relay_near(0)
    for k in far_order:
        settle_recv(xr.at[t, k], d_recv.at[k])
        for j in range(1, pairs):
            remote(
                xr.at[t, k], xr.at[t, k], x_send.at[0], x_recv.at[k - far, j - 1], {"tp": quarter_at(j)}
            ).start()
        to_sib(chunk_of[k], t, k)
    for k in near_order[::-1]:
        relay_near(k)

    def relay_far(c):
        for k in members(c):
            for j in range(1, pairs):
                settle_recv(xr.at[t, k], x_recv.at[k - far, j - 1])
                to_sib(c, lax.rem(t + T - 2 * j, T), k)

    def rows_of(blocks, c):
        return [
            blocks(k)[:, i * Q : (i + 1) * Q]
            for k in range(chunks[c][0], sum(chunks[c]))
            for i in range(FT)
        ]

    def folds_of(blocks, c):
        return [blocks(k)[:, FT * Q :] for k in range(chunks[c][0], sum(chunks[c]))]

    def experts(c):
        lo, n = chunks[c]
        settle_recv(xr.at[pl.ds(0, pairs), pl.ds(lo, n)], sib_recv.at[c])
        block = []
        folds = []
        for q in range(T):
            block.append(jnp.concatenate(rows_of(lambda k: xr.at[q, k], c), axis=0))
            if REST:
                for k in range(n):
                    fold = xr[q, lo + k, :, FT * Q :].astype(F32)
                    lines[c, q, pl.ds(k, QL, stride=SUB), :] = fold[:QL]
                folds += [lines[c, q, i * SUB : (i + 1) * SUB, :] for i in range(QL)]
        block = jnp.concatenate(block, axis=1)
        if REST:
            block = jnp.concatenate(
                [block, jnp.concatenate(folds, axis=1).astype(BF16)], axis=0
            )
        both = dot(block, wgu[...])
        gate = jnp.minimum(both[:, :F], clamp_limit)
        upward = jnp.clip(both[:, F:], -clamp_limit, clamp_limit)
        active = (upward + 1.0) * gate * (1.0 / (1.0 + jnp.exp(-sigmoid_alpha * gate)))
        active = active.astype(BF16)

        def down(quarter, step):
            cols = lanes_of(quarter)
            y = dot(active, wd[:, cols])
            for k in range(n):
                for i in range(FT):
                    at = (k * FT + i) * SUB
                    part[quarter, lo + k, :, i * Q : (i + 1) * Q] = y[at : at + SUB].astype(BF16)
            if REST:
                for i in range(QL):
                    folded[c, step, pl.ds(i, n, stride=SUB), :] = y[
                        n * FT * SUB : n * FT * SUB + n, i * LANES : (i + 1) * LANES
                    ]
                for k in range(n):
                    fold = folded[c, step, k * SUB : (k + 1) * SUB, :]
                    part[quarter, lo + k, :, FT * Q :] = fold.astype(BF16)

        for j in range(pairs - 1, -1, -1):
            quarter = lax.rem(sib + 2 * j, T)
            down(quarter, j)
            remote(
                part.at[quarter, pl.ds(lo, n)],
                s1.at[quarter, pl.ds(lo, n)],
                s1_send.at[0],
                s1_recv.at[c, j],
                {"tp": sib},
            ).start()
        for j in range(pairs - 1, -1, -1):
            down(quarter_at(j), pairs + j)

    def chip_sum(quarter, k):
        return part[quarter, k].astype(F32) + s1[quarter, k].astype(F32)

    def return_near():
        for j in range(pairs):
            settle_recv(s1.at[quarter_at(j), pl.ds(0, far)], s1_recv.at[0, j])
        for k in near_order:
            for j in range(pairs):
                rsend[j, k] = chip_sum(quarter_at(j), k).astype(BF16)
                remote(
                    rsend.at[j, k], ret.at[j, k], ret_send.at[1], ret_recv.at[1], {"ep": swap(k)}
                ).start()
        for j in range(pairs):
            ret[j, 0] = chip_sum(quarter_at(j), 0).astype(BF16)

    def reduce_far(c):
        lo, n = chunks[c]
        for j in range(pairs - 1, 0, -1):
            quarter = quarter_at(j)
            settle_recv(s1.at[quarter, pl.ds(lo, n)], s1_recv.at[c, j])
            for k in members(c):
                xsend[j, k] = chip_sum(quarter, k).astype(BF16)
                remote(
                    xsend.at[j, k],
                    xrecv.at[j, k],
                    rx_send.at[0],
                    rx_recv.at[k - far, j - 1],
                    {"tp": quarter},
                ).start()

    def return_far(c):
        lo, n = chunks[c]
        settle_recv(s1.at[t, pl.ds(lo, n)], s1_recv.at[c, 0])
        for k in members(c):
            total = chip_sum(t, k)
            for j in range(1, pairs):
                settle_recv(xrecv.at[j, k], rx_recv.at[k - far, j - 1])
                total = total + xrecv[j, k].astype(F32)
            rsend[0, k] = total.astype(BF16)
            remote(
                rsend.at[0, k], ret.at[0, k], ret_send.at[0], ret_recv.at[0], {"ep": swap(k)}
            ).start()

    def combine(j, c):
        rows = rows_of(lambda k: ret.at[j, k], c)
        if REST:
            n = chunks[c][1]
            fold = jnp.concatenate(folds_of(lambda k: ret.at[j, k], c), axis=0).astype(F32)
            line = lax.broadcasted_iota(jnp.int32, (n * SUB, LANES), 0) & (SUB - 1)
            lanes = [jnp.where(line == i, fold, 0.0).astype(BF16) for i in range(QL)]
            rows.append(jnp.concatenate(lanes, axis=1))
        rows = jnp.concatenate(rows, axis=0)
        return sum(dot(w, rows) for w in combines[c])

    arrive("wgu")
    arrive("wd")
    experts(0)
    relay_far(1)
    return_near()
    experts(1)
    reduce_far(1)
    return_far(1)
    settle_recv(ret.at[pl.ds(0, pairs), pl.ds(1, far - 1)], ret_recv.at[1])
    for j in range(pairs):
        nsend[:, j] = combine(j, 0).astype(BF16).reshape(T, RP, Q)
    scatter_tp(8, nsend, nrecv)
    settle_recv(ret.at[0, pl.ds(far, far)], ret_recv.at[0])
    far_part = sum(combine(0, c) for c in far_chunks)
    msend[...] = far_part.astype(BF16).reshape(T, RP, Q)
    scatter_tp(7, msend, mrecv)
    finish_tp(6, mxrecv)
    finish_tp(8, nrecv)
    finish_tp(7, mrecv)
    moe = []
    for q in range(T):
        total = mrecv[q].astype(F32)
        for j in range(pairs):
            total = total + nrecv[(q + T - 2 * j) % T, j].astype(F32)
        moe.append(total)
    moe = jnp.concatenate(moe, axis=1).astype(BF16).astype(F32)
    mixed_own = jnp.concatenate([mxrecv[s] for s in range(T)], axis=1).astype(F32)
    out_result[...] = (mixed_own + rms_scale(moe, gain(post_ffn_gain))).astype(BF16)[:R]

    fetch("out_result")
    for slot, view in sorted(sent_tp.items()):
        settle_send(view, tp_send.at[slot])
    settle_send(xr.at[0, pl.ds(0, far)], d_send.at[0])
    settle_send(xr.at[pl.ds(0, pairs), pl.ds(1, far - 1)], d_send.at[1])
    if pairs > 1:
        settle_send(aq.at[pl.ds(0, pairs - 1)], p_send.at[0])
        settle_send(xr.at[pl.ds(0, pairs - 1), pl.ds(0, far)], x_send.at[0])
        settle_send(xsend.at[pl.ds(1, pairs - 1), pl.ds(0, far)], rx_send.at[0])
    settle_send(xr.at[pl.ds(0, pairs)], sib_send.at[0])
    settle_send(part.at[pl.ds(0, pairs)], s1_send.at[0])
    settle_send(xr.at[0, pl.ds(0, far)], ret_send.at[0])
    settle_send(xr.at[pl.ds(0, pairs), pl.ds(1, far - 1)], ret_send.at[1])
    for name in ("out_rope", "out_latent", "out_result"):
        arrive(name)


def hand_over(result, latent, rope, out_result, out_latent, out_rope):
    out_result[...] = result[...]
    out_latent[...] = latent[...]
    out_rope[...] = rope[...]


def body(
    tokens,
    cache_latent,
    cache_rope,
    lengths,
    attn_gain,
    latent_gain,
    post_attn_gain,
    ffn_gain,
    post_ffn_gain,
    w_query,
    w_query_rot,
    w_latent,
    w_key_rot,
    w_key_up,
    w_value_up,
    w_out,
    route_logits,
    routes,
    w_gate,
    w_up,
    w_down,
):
    R, D = tokens.shape
    T = lax.axis_size("tp")
    EP = lax.axis_size("ep")
    C, LH, KD = w_key_up.shape
    RD = w_key_rot.shape[1]
    VD = w_value_up.shape[2]
    H = T * LH
    K = routes.shape[1]
    scale = (KD + RD) ** (-0.5)
    RP = 2 * SUB
    assert R == SUB + SUB // 2 and T % 2 == 0 and LH % 2 == 0
    assert EP & (EP - 1) == 0 and T * R <= LANES
    cap = (R * T * K + EP - 1) // EP + 1
    Q = D // T
    F = w_gate.shape[2]
    LC = w_latent.shape[1]
    SPAN = cache_latent.shape[1]
    N = T * R
    QL = Q // LANES
    FT, REST = cap // SUB, cap % SUB
    if REST > 1 or QL > SUB:
        FT, REST = -(-cap // SUB), 0
    W = FT * Q + REST * LANES
    far = EP // 2
    chunks = ((0, far), (far, far))
    table, places = layout(T, R, LH, chunks, FT, REST, QL)

    vm = pl.BlockSpec(memory_space=pltpu.VMEM)
    hbm = pl.BlockSpec(memory_space=pl.ANY)
    dma = pltpu.SemaphoreType.DMA
    pairs = T // 2
    ROT = LH * RD
    QW = (LH + LH // 2) * C + ROT + LC + ROT // 2 + LC

    def v(*shape, dtype=BF16):
        return pltpu.VMEM(shape, dtype)

    cfg = (T, EP, R, LH, FT, REST, chunks, scale, places)
    outs = pl.pallas_call(
        functools.partial(kernel, cfg),
        out_shape=(
            jax.ShapeDtypeStruct((R, D), BF16),
            jax.ShapeDtypeStruct((R, C), BF16),
            jax.ShapeDtypeStruct((R, RD), BF16),
        ),
        in_specs=[hbm] * 22,
        out_specs=(hbm, hbm, hbm),
        scratch_shapes=[
            pltpu.SMEM((R,), jnp.int32),
            v(R, D),
            v(D),
            v(C),
            v(D),
            v(D),
            v(D),
            v(K, N, dtype=jnp.int32),
            v(K, N, dtype=F32),
            v(R, D),
            v(R, C),
            v(R, RD),
            v(*table.shape),
            v(R, SPAN, C),
            v(R, RD, SPAN),
            v(D, LH * KD + ROT + LC),
            v(RD, D),
            v(C, LH * KD),
            v(C, LH * VD),
            v(LH * VD, D),
            v(D, 2 * F),
            v(F, D),
            v(T, SUB, D + D // 2),
            v(N, D),
            v(SUB, D, dtype=F32),
            v(T, SUB, QW),
            v(T, SUB, QW),
            v(R, H, C),
            v(R, H, RD),
            v(RP, C, dtype=F32),
            v(RP, RD, dtype=F32),
            v(R, H, C),
            v(T, SUB * LH, C),
            v(T, SUB * LH, C),
            v(T, (R - SUB) * LH, C),
            v(T, (R - SUB) * LH, C),
            v(T, N, Q),
            v(T, N, Q),
            v(T, N, Q),
            v(T, SUB, LANES, dtype=F32),
            v(T, RP, Q),
            v(T, RP, Q),
            v(pairs, EP, SUB, W),
            v(T, EP, SUB, W),
            v(T, EP, SUB, W),
            v(T, EP, SUB, W),
            v(pairs, EP, SUB, W),
            v(pairs, EP, SUB, W),
            v(pairs, EP, SUB, W),
            v(pairs, EP, SUB, W),
            v(T, RP, Q),
            v(T, RP, Q),
            v(T, pairs, RP, Q),
            v(T, pairs, RP, Q),
            v(len(chunks), T, QL * SUB, LANES, dtype=F32),
            v(len(chunks), T, far * SUB, LANES, dtype=F32),
            v(C, LH, KD),
            v(C, LH, VD),
            v(C * LH, KD, dtype=F32),
            v(R, H, SPAN, dtype=F32),
            v(R, H, SPAN),
            dma((19,)),
            dma((3,)),
            dma((10,)),
            dma((1,)),
            dma((pairs,)),
            dma((2,)),
            dma((EP,)),
            dma((1,)),
            dma((far, max(1, pairs - 1))),
            dma((1,)),
            dma((len(chunks),)),
            dma((1,)),
            dma((len(chunks), pairs)),
            dma((1,)),
            dma((far, max(1, pairs - 1))),
            dma((2,)),
            dma((2,)),
            pltpu.SemaphoreType.REGULAR((max(1, EP.bit_length() - 2),)),
        ],
        compiler_params=pltpu.CompilerParams(
            collective_id=0, has_side_effects=True, vmem_limit_bytes=60 * 1024 * 1024
        ),
    )(
        lengths,
        tokens,
        attn_gain,
        latent_gain,
        post_attn_gain,
        ffn_gain,
        post_ffn_gain,
        routes.T,
        route_logits.T,
        jnp.asarray(table, BF16),
        cache_latent,
        cache_rope,
        w_query,
        w_query_rot,
        w_latent,
        w_key_rot.T,
        w_key_up,
        w_value_up,
        w_out,
        w_gate,
        w_up,
        w_down,
    )
    return pl.pallas_call(
        hand_over,
        out_shape=tuple(jax.ShapeDtypeStruct(o.shape, o.dtype) for o in outs),
        in_specs=[vm] * 3,
        out_specs=(vm, vm, vm),
    )(*outs)


def solution(mesh):
    return jax.shard_map(
        body,
        mesh=mesh,
        in_specs=(
            P(("ep", "tp"), None),
            P(("ep", "tp"), None, None),
            P(("ep", "tp"), None, None),
            P(("ep", "tp")),
            P(),
            P(),
            P(),
            P(),
            P(),
            P(None, "tp"),
            P(None, "tp"),
            P(None, "tp"),
            P(),
            P(None, "tp", None),
            P(None, "tp", None),
            P("tp", None),
            P("ep", None),
            P("ep", None),
            P("ep", None, "tp"),
            P("ep", None, "tp"),
            P("ep", "tp", None),
        ),
        out_specs=(P(("ep", "tp"), None), P(("ep", "tp"), None), P(("ep", "tp"), None)),
        check_vma=False,
    )
```

```python
import functools

import jax
import jax.numpy as jnp
import numpy as np
from jax import lax
from jax.experimental import pallas as pl
from jax.experimental.pallas import tpu as pltpu
from jax.sharding import PartitionSpec as P

eps_norm = 1e-06
clamp_limit = 7.0
sigmoid_alpha = 1.702
theta_base = 10000.0
MESH = pl.DeviceIdType.MESH
F32 = jnp.float32
BF16 = jnp.bfloat16
SUB = 8
LANES = 128


def rms_scale(values, gain):
    mean_square = jnp.mean(values * values, axis=-1, keepdims=True)
    return values * lax.rsqrt(mean_square + eps_norm) * gain


def turn(values, cosine, sine):
    half = values.shape[-1] // 2
    swapped = jnp.concatenate([values[:, half:], values[:, :half]], axis=1)
    return values * cosine + swapped * sine


def dot(a, b):
    return jnp.dot(a, b, preferred_element_type=F32)


def dot_nt(a, b):
    return lax.dot_general(a, b, (((1,), (1,)), ((), ())), preferred_element_type=F32)


def remote(src, dst, send_sem, recv_sem, where):
    return pltpu.make_async_remote_copy(
        src_ref=src,
        dst_ref=dst,
        send_sem=send_sem,
        recv_sem=recv_sem,
        device_id=where,
        device_id_type=MESH,
    )


def half_rows(values):
    return lax.broadcasted_iota(jnp.int32, values.shape, 0) < SUB // 2


def join_halves(upper, lower):
    return jnp.where(half_rows(upper), upper, pltpu.roll(lower, SUB // 2, 0))


def join_ends(upper, lower):
    return jnp.where(half_rows(upper), pltpu.roll(upper, SUB // 2, 0), lower)


def layout(T, R, LH, chunks, FT, REST, QL):
    H = T * LH
    tail = R - SUB
    mid = LH // 2

    def packed(s, b):
        if b < SUB:
            return s * SUB + b
        return T * SUB + (s // 2) * SUB + (s % 2) * tail + b - SUB

    to_seq = np.zeros((SUB * H, H * SUB))
    to_seq_tail = np.zeros((tail * H, T * mid * SUB))
    to_turn_tail = np.zeros((tail * H, T * mid * SUB))
    to_head = np.zeros((H * SUB, SUB * H))
    to_head_tail = np.zeros((H * tail, tail * H))
    to_value = np.zeros((LH * T * R, LH * T * R))
    for s in range(T):
        for h in range(LH):
            head = s * LH + h
            for b in range(SUB):
                to_seq[b * H + head, head * SUB + b] = 1
                to_head[head * SUB + b, b * H + head] = 1
                to_value[h * T * R + packed(s, b), head * SUB + b] = 1
            for b in range(tail):
                at = (s * mid + h // 2) * SUB + (h % 2) * tail + b
                to_seq_tail[b * H + head, at] = 1
                at = (s * mid + h % mid) * SUB + (h // mid) * tail + b
                to_turn_tail[b * H + head, at] = 1
                to_head_tail[head * tail + b, b * H + head] = 1
                at = H * SUB + head * tail + b
                to_value[h * T * R + packed(s, SUB + b), at] = 1
    spread = np.zeros((T * R, T * R))
    own_natural = np.zeros((T * 2 * SUB, T * R))
    own_packed = np.zeros((T * 2 * SUB, T * R))
    for s in range(T):
        for b in range(R):
            spread[packed(s, b), s * R + b] = 1
            own_natural[s * 2 * SUB + b, s * R + b] = 1
            own_packed[s * 2 * SUB + b, packed(s, b)] = 1
    groups, slots = [], []
    for lo, n in chunks:
        for k in range(n):
            groups += [lo + k] * (FT * SUB)
            slots += range(FT * SUB)
        for k in range(n if REST else 0):
            groups += [lo + k] * SUB
            slots += [FT * SUB] * QL + [-1] * (SUB - QL)
    group_of = np.repeat(np.array(groups)[:, None], T * R, 1)
    slot_of = np.repeat(np.array(slots)[:, None], T * R, 1)
    parts = [to_seq, to_seq_tail, to_turn_tail, to_value, spread, own_natural, own_packed]
    parts += [group_of, slot_of, to_head, to_head_tail]
    width = max(p.shape[1] for p in parts)
    rows, places = 0, []
    for p in parts:
        places.append((rows, p.shape[0], p.shape[1]))
        rows += -(-p.shape[0] // 16) * 16
    table = np.zeros((rows, width), np.float32)
    for p, (row, n, m) in zip(parts, places):
        table[row : row + n, :m] = p
    return table, tuple(places)


def kernel(
    cfg,
    lengths_h,
    tokens_h,
    attn_gain_h,
    latent_gain_h,
    post_attn_gain_h,
    ffn_gain_h,
    post_ffn_gain_h,
    routes_t_h,
    logits_t_h,
    table_h,
    cache_h,
    rope_h,
    wq_h,
    wqr_h,
    wl_h,
    wkr_h,
    wku_h,
    wvu_h,
    wo_h,
    wg_h,
    wu_h,
    wd_h,
    out_result_h,
    out_latent_h,
    out_rope_h,
    lengths,
    tokens,
    attn_gain,
    latent_gain,
    post_attn_gain,
    ffn_gain,
    post_ffn_gain,
    routes_t,
    logits_t,
    out_result,
    out_latent,
    out_rope,
    table,
    cache,
    rope,
    wall,
    wkr,
    wku,
    wvu,
    wo,
    wgu,
    wd,
    xg,
    rows_all,
    gains,
    qsend,
    qrecv,
    qs,
    qt,
    nlat,
    nrope,
    hl,
    hsend,
    hrecv,
    hsend_tail,
    hrecv_tail,
    asend,
    arecv,
    aq,
    srecv,
    mxsend,
    mxrecv,
    sl,
    xr,
    part,
    s1,
    xsend,
    xrecv,
    rsend,
    ret,
    msend,
    mrecv,
    nsend,
    nrecv,
    lines,
    folded,
    ku3,
    vu3,
    wide,
    sc,
    pb,
    w_sem,
    tp_send,
    tp_recv,
    p_send,
    p_recv,
    d_send,
    d_recv,
    x_send,
    x_recv,
    sib_send,
    sib_recv,
    s1_send,
    s1_recv,
    rx_send,
    rx_recv,
    ret_send,
    ret_recv,
    met,
):
    T, EP, R, LH, FT, REST, chunks, scale, places = cfg
    H = T * LH
    t = lax.axis_index("tp")
    e = lax.axis_index("ep")
    C = wku.shape[0]
    KD = wku.shape[1] // LH
    RD = wkr.shape[0]
    VD = wvu.shape[1] // LH
    D, WA = wall.shape
    F = wd.shape[0]
    LC = WA - LH * KD - LH * RD
    Q = D // T
    N = T * R
    RP = 2 * SUB
    QL = Q // LANES
    W = xr.shape[3]
    SPAN = cache.shape[1]
    tail = R - SUB
    mid = LH // 2
    FOLD = D // 2
    pairs = T // 2
    sib = t + 1 - 2 * lax.rem(t, 2)

    def one_hot(i):
        row, n, m = places[i]
        return table[row : row + n, :m]

    def swap(k):
        other = e
        bit = 1
        while bit < EP:
            if k & bit:
                other = other + bit - 2 * bit * lax.rem(lax.div(e, bit), 2)
            bit *= 2
        return other

    loads = {}
    for i, (name, copies) in enumerate(
        [
            (
                "wall",
                [
                    (wq_h, wall.at[:, : LH * KD]),
                    (wqr_h, wall.at[:, LH * KD : LH * KD + LH * RD]),
                    (wl_h, wall.at[:, LH * KD + LH * RD :]),
                ],
            ),
            ("wkr", [(wkr_h, wkr)]),
            ("wku", [(wku_h, ku3)]),
            ("wvu", [(wvu_h, vu3)]),
            ("wo", [(wo_h, wo)]),
            ("wgu", [(wg_h.at[0], wgu.at[:, :F]), (wu_h.at[0], wgu.at[:, F:])]),
            ("wd", [(wd_h.at[0], wd)]),
            ("table", [(table_h, table)]),
            ("cache", [(cache_h.at[b], cache.at[b]) for b in range(R)]),
            ("rope", [(rope_h, rope)]),
            ("tokens", [(tokens_h, tokens)]),
            ("lengths", [(lengths_h, lengths)]),
            ("attn_gain", [(attn_gain_h, attn_gain)]),
            ("latent_gain", [(latent_gain_h, latent_gain)]),
            ("post_attn_gain", [(post_attn_gain_h, post_attn_gain)]),
            ("ffn_gain", [(ffn_gain_h, ffn_gain)]),
            ("post_ffn_gain", [(post_ffn_gain_h, post_ffn_gain)]),
            ("routes", [(routes_t_h, routes_t)]),
            ("logits", [(logits_t_h, logits_t)]),
        ]
    ):
        loads[name] = (i, copies)
    for name, copies in (
        ("out_rope", (out_rope, out_rope_h)),
        ("out_latent", (out_latent, out_latent_h)),
        ("out_result", (out_result, out_result_h)),
    ):
        earlier = {"out_rope": "tokens", "out_latent": "wall", "out_result": "wkr"}[name]
        loads[name] = (loads[earlier][0], [copies])
    whole = {"wall": wall, "wgu": wgu, "cache": cache}

    def fetch(name):
        i, copies = loads[name]
        for src, dst in copies:
            pltpu.make_async_copy(src, dst, w_sem.at[i]).start()

    def arrive(name):
        i, copies = loads[name]
        src, dst = (whole[name], whole[name]) if name in whole else copies[0]
        pltpu.make_async_copy(src, dst, w_sem.at[i]).wait()

    fetch("tokens")
    barrier = pltpu.get_barrier_semaphore()
    for k in range(1, T):
        pl.semaphore_signal(
            barrier, inc=1, device_id={"tp": lax.rem(t + k, T)}, device_id_type=MESH
        )
    bits = [1 << i for i in range(EP.bit_length() - 1)]

    def greet(sem):
        for k in bits:
            pl.semaphore_signal(sem, inc=1, device_id={"ep": swap(k)}, device_id_type=MESH)

    greet(barrier)
    for name in ("attn_gain", "lengths", "post_attn_gain", "ffn_gain", "latent_gain"):
        fetch(name)
    for name in ("wku", "wkr", "wall", "table", "post_ffn_gain", "routes", "logits"):
        fetch(name)

    def gain(ref):
        return ref[...].astype(F32)[None, :]

    def by_head_columns(source, target):
        size = source.shape[2]
        wide[...] = source[...].astype(F32).reshape(C * LH, size)
        for h in range(LH):
            target[:, h * size : (h + 1) * size] = wide[pl.ds(h, C, stride=LH), :].astype(BF16)

    def settle_recv(ref, sem):
        remote(ref, ref, sem, sem, {"tp": sib}).wait_recv()

    def settle_send(ref, sem):
        remote(ref, ref, sem, sem, {"tp": sib}).wait_send()

    sent_tp = {}
    send_of = {0: 0, 1: 1, 9: 2, 2: 0, 3: 1, 4: 2, 5: 0, 6: 1, 8: 2, 7: 0}

    def reuse_send(phase):
        slot = send_of[phase]
        if slot in sent_tp:
            settle_send(sent_tp.pop(slot), tp_send.at[slot])
        return tp_send.at[slot]

    peers = [lax.rem(c + 2 * j, T) for c in (t, sib) for j in range(1, pairs)] + [sib]

    def gather_tp(phase, src, dst):
        sent = reuse_send(phase)
        for peer in peers:
            remote(
                src, dst.at[t], sent, tp_recv.at[phase], {"tp": peer}
            ).start()

    def scatter_tp(phase, src, dst):
        sent = reuse_send(phase)
        for peer in peers:
            remote(
                src.at[peer], dst.at[t], sent, tp_recv.at[phase], {"tp": peer}
            ).start()
        dst[t] = src[t]


    def finish_tp(phase, dst, lanes=None):
        view = dst.at[pl.ds(0, T - 1)] if lanes is None else dst.at[pl.ds(0, T - 1), :, lanes]
        settle_recv(view, tp_recv.at[phase])
        sent_tp[send_of[phase]] = view

    arrive("tokens")
    token_values = jnp.concatenate(
        [tokens[...].astype(F32), jnp.zeros((RP - R, D), F32)], axis=0
    )
    left, right = token_values[SUB:, :FOLD], token_values[SUB:, FOLD:]
    xg[t] = jnp.concatenate(
        [token_values[:SUB], join_halves(left, right)], axis=1
    ).astype(BF16)
    pl.semaphore_wait(barrier, T - 1 + len(bits))

    gather_tp(0, xg.at[t], xg)
    fetch("cache")
    fetch("rope")
    greet(met.at[0])
    for name in ("attn_gain", "lengths", "post_attn_gain", "ffn_gain"):
        arrive(name)
    own_normed = rms_scale(token_values, gain(attn_gain)).astype(BF16)
    for i, ref in enumerate((post_attn_gain, ffn_gain)):
        gains[i : i + 1, :] = gain(ref)
    half = RD // 2
    lane = lax.broadcasted_iota(jnp.int32, (RP, RD), 1)
    row = lax.broadcasted_iota(jnp.int32, (RP, RD), 0)
    freqs = jnp.zeros((RP, RD), F32)
    for i in range(half):
        hit = (lane == i) | (lane == i + half)
        freqs = jnp.where(hit, np.float32(theta_base ** (-i / half)), freqs)
    positions = jnp.zeros((RP, RD), jnp.int32)
    for b in range(R):
        positions = jnp.where(row == b, lengths[b], positions)
    angles = positions.astype(F32) * freqs
    cosine = jnp.cos(angles)
    sine = jnp.sin(angles)
    sine = jnp.where(lane < half, -sine, sine)
    arrive("wku")
    by_head_columns(ku3, wku)
    arrive("wkr")
    key_raw = dot_nt(own_normed, wkr[...]).astype(BF16).astype(F32)
    new_rope = turn(key_raw, cosine, sine).astype(BF16)
    nrope[...] = new_rope.astype(F32)
    out_rope[...] = new_rope[:R]
    fetch("out_rope")
    arrive("wall")
    arrive("table")
    finish_tp(0, xg)

    blocks = [xg[s, :, :D].astype(F32) for s in range(T)]
    for p in range(pairs):
        first = xg[2 * p, :, D:].astype(F32)
        second = xg[2 * p + 1, :, D:].astype(F32)
        blocks.append(
            jnp.concatenate([join_halves(first, second), join_ends(first, second)], axis=1)
        )
    rows = jnp.concatenate(blocks, axis=0)
    rows_all[...] = rows.astype(BF16)
    row_square = jnp.sum(rows * rows, axis=1, keepdims=True)
    normed = (rows * lax.rsqrt(row_square * (1.0 / D) + eps_norm) * gain(attn_gain)).astype(BF16)
    projected = dot(normed, wall[...])
    plain = projected[:, : LH * KD].astype(BF16)
    extra = projected[:, LH * KD :]
    lifted = [
        dot_nt(plain[:, h * KD : (h + 1) * KD], wku[:, h * KD : (h + 1) * KD])
        for h in range(LH)
    ]
    ROT = LH * RD
    split = LH * C + ROT + LC
    turn_tail = split + mid * C
    early, late = pl.ds(0, split), pl.ds(split, qsend.shape[2] - split)

    def send_queries(phase, lanes):
        sent = reuse_send(phase)
        for peer in peers:
            remote(
                qsend.at[peer, :, lanes],
                qrecv.at[t, :, lanes],
                sent,
                tp_recv.at[phase],
                {"tp": peer},
            ).start()

    for s in range(T):
        top = slice(s * SUB, (s + 1) * SUB)
        for h in range(LH):
            qsend[s, :, h * C : (h + 1) * C] = lifted[h][top].astype(BF16)
        qsend[s, :, LH * C : split] = extra[top].astype(BF16)
    send_queries(1, early)
    for s in range(T):
        join = join_halves if s % 2 == 0 else join_ends
        rest = slice(T * SUB + (s // 2) * SUB, T * SUB + (s // 2 + 1) * SUB)
        for h in range(0, LH, 2):
            at = split + (h // 2) * C
            qsend[s, :, at : at + C] = join(lifted[h][rest], lifted[h + 1][rest]).astype(BF16)
        last = extra[rest]
        at = turn_tail
        qsend[s, :, at : at + ROT // 2] = join(
            last[:, : ROT // 2], last[:, ROT // 2 : ROT]
        ).astype(BF16)
        at += ROT // 2
        last = last[:, ROT:]
        qsend[s, :, at : at + LC] = join(last, last).astype(BF16)
    send_queries(9, late)
    qrecv[t] = qsend[t]
    for name in ("wvu", "wo", "wgu", "wd"):
        fetch(name)
    for i in range(1, len(bits)):
        pl.semaphore_wait(met.at[i - 1], len(bits))
        if i < len(bits) - 1:
            greet(met.at[i])
    finish_tp(1, qrecv, early)

    arrive("latent_gain")

    def fresh_latent(at):
        raw = jnp.concatenate([qrecv[s, :, at : at + LC] for s in range(T)], axis=1)
        return rms_scale(raw.astype(F32), gain(latent_gain)).astype(BF16)

    def queries(first, table_of, blocks):
        stacked = jnp.concatenate(blocks, axis=0)
        rows = dot(table_of, stacked).astype(BF16)
        return rows.reshape(first, H, stacked.shape[1])

    def turned(at, count, cosine, sine):
        return [
            turn(qrecv[s, :, at + i * RD : at + (i + 1) * RD].astype(F32), cosine, sine).astype(BF16)
            for s in range(T)
            for i in range(count)
        ]

    def blocks_of(at, count):
        return [qrecv[s, :, at + i * C : at + (i + 1) * C] for s in range(T) for i in range(count)]

    latent = fresh_latent(LH * C + ROT)
    out_latent[:SUB] = latent
    nlat[:SUB] = latent.astype(F32)
    qs[:SUB] = queries(SUB, one_hot(0), blocks_of(0, LH))
    qt[:SUB] = queries(SUB, one_hot(0), turned(LH * C, LH, cosine[:SUB], sine[:SUB]))

    def late_queries():
        finish_tp(9, qrecv, late)
        latent = fresh_latent(turn_tail + ROT // 2)
        out_latent[SUB:] = latent[:tail]
        fetch("out_latent")
        nlat[SUB:] = latent.astype(F32)
        qs[SUB:] = queries(tail, one_hot(1), blocks_of(split, mid))
        cos, sin = cosine[SUB:], sine[SUB:]
        cos, sin = join_halves(cos, cos), join_halves(sin, sin)
        qt[SUB:] = queries(tail, one_hot(2), turned(turn_tail, mid, cos, sin))

    arrive("cache")
    arrive("rope")
    position = lax.broadcasted_iota(jnp.int32, (H, SPAN), 1)
    for members, table_of, phase, send, recv in (
        (range(SUB), one_hot(9), 2, hsend, hrecv),
        (range(SUB, R), one_hot(10), 3, hsend_tail, hrecv_tail),
    ):
        if phase == 3:
            late_queries()
        for b in members:
            scores = (dot_nt(qs[b], cache[b]) + dot(qt[b], rope[b])) * scale
            sc[b] = jnp.where(position < lengths[b], scores, -jnp.inf)
        prob_own = {}
        for b in members:
            own = (
                jnp.sum(qs[b].astype(F32) * nlat[b : b + 1, :], axis=1, keepdims=True)
                + jnp.sum(qt[b].astype(F32) * nrope[b : b + 1, :], axis=1, keepdims=True)
            ) * scale
            masked = sc[b]
            highest = jnp.maximum(jnp.max(masked, axis=1, keepdims=True), own)
            raised = jnp.exp(masked - highest)
            raised_own = jnp.exp(own - highest)
            inverse = 1.0 / (jnp.sum(raised, axis=1, keepdims=True) + raised_own)
            pb[b] = (raised * inverse).astype(BF16)
            prob_own[b] = (raised_own * inverse).astype(BF16).astype(F32)
        for b in members:
            hl[b] = (dot(pb[b], cache[b]) + prob_own[b] * nlat[b : b + 1, :]).astype(BF16)
        count = len(members)
        attended = hl[members[0] : members[0] + count].reshape(count * H, C)
        send[...] = dot(table_of, attended).astype(BF16).reshape(T, count * LH, C)
        scatter_tp(phase, send, recv)

    lines[...] = jnp.zeros_like(lines)
    folded[...] = jnp.zeros_like(folded)
    for name in ("routes", "logits", "post_ffn_gain", "wvu"):
        arrive(name)
    by_head_columns(vu3, wvu)
    arrive("wo")
    group_of = one_hot(7).astype(F32).astype(jnp.int32) ^ e
    slot_of = one_hot(8).astype(F32)
    gi = lax.broadcasted_iota(jnp.int32, (N, N), 0)
    gj = lax.broadcasted_iota(jnp.int32, (N, N), 1)
    upper = (gi < gj).astype(F32).astype(BF16)
    lg = logits_t[...]
    lg = jnp.exp(lg - jnp.max(lg, axis=0, keepdims=True))
    weights = lg / jnp.sum(lg, axis=0, keepdims=True)
    count = jnp.zeros(slot_of.shape, F32)
    weighted = jnp.zeros(slot_of.shape, F32)
    for k in range(routes_t.shape[0]):
        hit = routes_t[k : k + 1, :] == group_of
        count = jnp.where(hit, 1.0, count)
        weighted = jnp.where(hit, weights[k : k + 1, :], weighted)
    rank = dot(count.astype(BF16), upper)
    taken = rank == slot_of
    weighted = jnp.where(taken, weighted, 0.0)
    weighted_hi = weighted.astype(BF16)
    weighted_lo = (weighted - weighted_hi.astype(F32)).astype(BF16)
    dispatch = dot_nt(jnp.where(taken, count, 0.0).astype(BF16), one_hot(4)).astype(BF16)
    spans, combines = [], []
    for lo, n in chunks:
        first = spans[-1][1] if spans else 0
        spans.append((first, first + n * (FT + REST) * SUB))
        span = slice(*spans[-1])
        combines.append(
            [dot_nt(one_hot(5), w[span]).astype(BF16) for w in (weighted_hi, weighted_lo)]
        )

    finish_tp(2, hrecv)
    finish_tp(3, hrecv_tail)
    attended = jnp.concatenate(
        [hrecv[...].reshape(H * SUB, C), hrecv_tail[...].reshape(H * tail, C)], axis=0
    )
    heads = dot(one_hot(3), attended).astype(BF16)
    values = jnp.concatenate(
        [
            dot(heads[h * N : (h + 1) * N], wvu[:, h * VD : (h + 1) * VD]).astype(BF16)
            for h in range(LH)
        ],
        axis=1,
    )

    def lanes_of(quarter):
        return pl.ds(pl.multiple_of(quarter * Q, Q), Q)

    sent = reuse_send(4)
    for peer in peers:
        asend[peer] = dot(values, wo[:, lanes_of(peer)]).astype(BF16)
        remote(
            asend.at[peer], arecv.at[t], sent, tp_recv.at[4], {"tp": peer}
        ).start()
    arecv[t] = dot(values, wo[:, lanes_of(t)]).astype(BF16)
    finish_tp(4, arecv)
    attn = arecv[0].astype(F32)
    for s in range(1, T):
        attn = attn + arecv[s].astype(F32)
    aq[t] = attn.astype(BF16)
    attn = attn.astype(BF16).astype(F32)

    def row_sum(v):
        return jnp.sum(v, axis=1, keepdims=True)

    def scaled_branch(attn, quarter):
        own_tokens = rows_all[:, lanes_of(quarter)].astype(F32)
        return own_tokens, attn * gains[0:1, lanes_of(quarter)]

    own_tokens, scaled = scaled_branch(attn, t)
    at_lane = lax.broadcasted_iota(jnp.int32, (N, LANES), 1)
    sums = jnp.where(at_lane == 0, row_sum(attn * attn), 0.0)
    sums = jnp.where(at_lane == 1, row_sum(own_tokens * scaled), sums)
    sums = jnp.where(at_lane == 2, row_sum(scaled * scaled), sums)
    sums = jnp.concatenate([sums, jnp.zeros((LANES - N, LANES), F32)], axis=0)
    srecv[t] = sums.T[:SUB]
    gather_tp(5, srecv.at[t], srecv)
    for j in range(1, pairs):
        remote(
            aq.at[t], aq.at[t], p_send.at[0], p_recv.at[j], {"tp": lax.rem(t + 2 * j, T)}
        ).start()
    finish_tp(5, srecv)
    totals = srecv[0]
    for s in range(1, T):
        totals = totals + srecv[s]
    totals = jnp.concatenate([totals, jnp.zeros((LANES - SUB, LANES), F32)], axis=0).T[:N]
    inverse = lax.rsqrt(totals[:, 0:1] * (1.0 / D) + eps_norm)
    square = row_square + 2.0 * inverse * totals[:, 1:2] + inverse * inverse * totals[:, 2:3]
    square = jnp.maximum(square, 0.0)
    ffn_inverse = lax.rsqrt(square * (1.0 / D) + eps_norm)

    def ffn_rows(own_tokens, scaled, quarter):
        mixed = (own_tokens + scaled * inverse).astype(BF16)
        normed = mixed.astype(F32) * ffn_inverse * gains[1:2, lanes_of(quarter)]
        return mixed, normed.astype(BF16)

    order = sorted(range(1, EP), key=lambda k: (-k.bit_length(), k ^ 1, k))
    far = EP // 2
    far_order, near_order = order[:far], order[far:]

    def quarter_at(j):
        return lax.rem(t + 2 * j, T)

    def pack_slots(j, c, normed):
        lo, n = chunks[c]
        picked = dot(dispatch[slice(*spans[c])], normed)
        for k in range(n):
            for i in range(FT):
                at = (k * FT + i) * SUB
                sl[j, lo + k, :, i * Q : (i + 1) * Q] = picked[at : at + SUB].astype(BF16)
        if REST:
            rest = picked[n * FT * SUB :]
            line = lax.broadcasted_iota(jnp.int32, (n * SUB, LANES), 0) & (SUB - 1)
            fold = jnp.zeros((n * SUB, LANES), F32)
            for i in range(QL):
                fold = jnp.where(line == i, rest[:, i * LANES : (i + 1) * LANES], fold)
            for k in range(n):
                sl[j, lo + k, :, FT * Q :] = fold[k * SUB : (k + 1) * SUB].astype(BF16)

    mixed, normed = ffn_rows(own_tokens, scaled, t)
    for c in range(1, len(chunks)):
        pack_slots(0, c, normed)
    for k in far_order:
        remote(sl.at[0, k], xr.at[t, k], d_send.at[0], d_recv.at[k], {"ep": swap(k)}).start()

    def send_near(j):
        for k in near_order:
            remote(
                sl.at[j, k], xr.at[quarter_at(j), k], d_send.at[1], d_recv.at[k], {"ep": swap(k)}
            ).start()
        xr[quarter_at(j), 0] = sl[j, 0]

    pack_slots(0, 0, normed)
    send_near(0)
    for j in range(1, pairs):
        settle_recv(aq.at[0], p_recv.at[pairs - j])
        other = quarter_at(j)
        _, normed = ffn_rows(*scaled_branch(aq[other].astype(F32), other), other)
        pack_slots(j, 0, normed)
        send_near(j)

    chunk_of = {lo + k: c for c, (lo, n) in enumerate(chunks) for k in range(n)}
    far_chunks = range(1, len(chunks))

    def members(c):
        lo, n = chunks[c]
        return [k for k in order + [0] if lo <= k < lo + n]

    def to_sib(c, quarter, k):
        remote(
            xr.at[quarter, k], xr.at[quarter, k], sib_send.at[0], sib_recv.at[c], {"tp": sib}
        ).start()

    def relay_near(k):
        if k:
            settle_recv(xr.at[pl.ds(0, pairs), k], d_recv.at[k])
        for j in range(pairs):
            to_sib(0, quarter_at(j), k)

    relay_near(0)
    for k in far_order:
        settle_recv(xr.at[t, k], d_recv.at[k])
        for j in range(1, pairs):
            remote(
                xr.at[t, k], xr.at[t, k], x_send.at[0], x_recv.at[k - far, j - 1], {"tp": quarter_at(j)}
            ).start()
        to_sib(chunk_of[k], t, k)
    for k in near_order[::-1]:
        relay_near(k)

    def relay_far(c):
        for k in members(c):
            for j in range(1, pairs):
                settle_recv(xr.at[t, k], x_recv.at[k - far, j - 1])
                to_sib(c, lax.rem(t + T - 2 * j, T), k)

    def rows_of(blocks, c):
        return [
            blocks(k)[:, i * Q : (i + 1) * Q]
            for k in range(chunks[c][0], sum(chunks[c]))
            for i in range(FT)
        ]

    def folds_of(blocks, c):
        return [blocks(k)[:, FT * Q :] for k in range(chunks[c][0], sum(chunks[c]))]

    def experts(c):
        lo, n = chunks[c]
        settle_recv(xr.at[pl.ds(0, pairs), pl.ds(lo, n)], sib_recv.at[c])
        block = []
        folds = []
        for q in range(T):
            block.append(jnp.concatenate(rows_of(lambda k: xr.at[q, k], c), axis=0))
            if REST:
                for k in range(n):
                    fold = xr[q, lo + k, :, FT * Q :].astype(F32)
                    lines[c, q, pl.ds(k, QL, stride=SUB), :] = fold[:QL]
                folds += [lines[c, q, i * SUB : (i + 1) * SUB, :] for i in range(QL)]
        block = jnp.concatenate(block, axis=1)
        if REST:
            block = jnp.concatenate(
                [block, jnp.concatenate(folds, axis=1).astype(BF16)], axis=0
            )
        both = dot(block, wgu[...])
        gate = jnp.minimum(both[:, :F], clamp_limit)
        upward = jnp.clip(both[:, F:], -clamp_limit, clamp_limit)
        active = (upward + 1.0) * gate * (1.0 / (1.0 + jnp.exp(-sigmoid_alpha * gate)))
        active = active.astype(BF16)

        def down(quarter, step):
            cols = lanes_of(quarter)
            y = dot(active, wd[:, cols])
            for k in range(n):
                for i in range(FT):
                    at = (k * FT + i) * SUB
                    part[quarter, lo + k, :, i * Q : (i + 1) * Q] = y[at : at + SUB].astype(BF16)
            if REST:
                for i in range(QL):
                    folded[c, step, pl.ds(i, n, stride=SUB), :] = y[
                        n * FT * SUB : n * FT * SUB + n, i * LANES : (i + 1) * LANES
                    ]
                for k in range(n):
                    fold = folded[c, step, k * SUB : (k + 1) * SUB, :]
                    part[quarter, lo + k, :, FT * Q :] = fold.astype(BF16)

        for j in range(pairs - 1, -1, -1):
            quarter = lax.rem(sib + 2 * j, T)
            down(quarter, j)
            remote(
                part.at[quarter, pl.ds(lo, n)],
                s1.at[quarter, pl.ds(lo, n)],
                s1_send.at[0],
                s1_recv.at[c, j],
                {"tp": sib},
            ).start()
        for j in range(pairs - 1, -1, -1):
            down(quarter_at(j), pairs + j)

    def chip_sum(quarter, k):
        return part[quarter, k].astype(F32) + s1[quarter, k].astype(F32)

    def return_near():
        for j in range(pairs):
            settle_recv(s1.at[quarter_at(j), pl.ds(0, far)], s1_recv.at[0, j])
        for k in near_order:
            for j in range(pairs):
                rsend[j, k] = chip_sum(quarter_at(j), k).astype(BF16)
                remote(
                    rsend.at[j, k], ret.at[j, k], ret_send.at[1], ret_recv.at[1], {"ep": swap(k)}
                ).start()
        for j in range(pairs):
            ret[j, 0] = chip_sum(quarter_at(j), 0).astype(BF16)

    def reduce_far(c):
        lo, n = chunks[c]
        for j in range(pairs - 1, 0, -1):
            quarter = quarter_at(j)
            settle_recv(s1.at[quarter, pl.ds(lo, n)], s1_recv.at[c, j])
            for k in members(c):
                xsend[j, k] = chip_sum(quarter, k).astype(BF16)
                remote(
                    xsend.at[j, k],
                    xrecv.at[j, k],
                    rx_send.at[0],
                    rx_recv.at[k - far, j - 1],
                    {"tp": quarter},
                ).start()

    def return_far(c):
        lo, n = chunks[c]
        settle_recv(s1.at[t, pl.ds(lo, n)], s1_recv.at[c, 0])
        for k in members(c):
            total = chip_sum(t, k)
            for j in range(1, pairs):
                settle_recv(xrecv.at[j, k], rx_recv.at[k - far, j - 1])
                total = total + xrecv[j, k].astype(F32)
            rsend[0, k] = total.astype(BF16)
            remote(
                rsend.at[0, k], ret.at[0, k], ret_send.at[0], ret_recv.at[0], {"ep": swap(k)}
            ).start()

    def combine(j, c):
        rows = rows_of(lambda k: ret.at[j, k], c)
        if REST:
            n = chunks[c][1]
            fold = jnp.concatenate(folds_of(lambda k: ret.at[j, k], c), axis=0).astype(F32)
            line = lax.broadcasted_iota(jnp.int32, (n * SUB, LANES), 0) & (SUB - 1)
            lanes = [jnp.where(line == i, fold, 0.0).astype(BF16) for i in range(QL)]
            rows.append(jnp.concatenate(lanes, axis=1))
        rows = jnp.concatenate(rows, axis=0)
        return sum(dot(w, rows) for w in combines[c])

    arrive("wgu")
    arrive("wd")
    experts(0)
    relay_far(1)
    return_near()
    mxsend[...] = dot(one_hot(6), mixed).astype(BF16).reshape(T, RP, Q)
    scatter_tp(6, mxsend, mxrecv)
    experts(1)
    reduce_far(1)
    return_far(1)
    settle_recv(ret.at[pl.ds(0, pairs), pl.ds(1, far - 1)], ret_recv.at[1])
    for j in range(pairs):
        nsend[:, j] = combine(j, 0).astype(BF16).reshape(T, RP, Q)
    scatter_tp(8, nsend, nrecv)
    settle_recv(ret.at[0, pl.ds(far, far)], ret_recv.at[0])
    far_part = sum(combine(0, c) for c in far_chunks)
    msend[...] = far_part.astype(BF16).reshape(T, RP, Q)
    scatter_tp(7, msend, mrecv)
    finish_tp(6, mxrecv)
    finish_tp(8, nrecv)
    finish_tp(7, mrecv)
    moe = []
    for q in range(T):
        total = mrecv[q].astype(F32)
        for j in range(pairs):
            total = total + nrecv[(q + T - 2 * j) % T, j].astype(F32)
        moe.append(total)
    moe = jnp.concatenate(moe, axis=1).astype(BF16).astype(F32)
    mixed_own = jnp.concatenate([mxrecv[s] for s in range(T)], axis=1).astype(F32)
    out_result[...] = (mixed_own + rms_scale(moe, gain(post_ffn_gain))).astype(BF16)[:R]

    fetch("out_result")
    for slot, view in sorted(sent_tp.items()):
        settle_send(view, tp_send.at[slot])
    settle_send(xr.at[0, pl.ds(0, far)], d_send.at[0])
    settle_send(xr.at[pl.ds(0, pairs), pl.ds(1, far - 1)], d_send.at[1])
    if pairs > 1:
        settle_send(aq.at[pl.ds(0, pairs - 1)], p_send.at[0])
        settle_send(xr.at[pl.ds(0, pairs - 1), pl.ds(0, far)], x_send.at[0])
        settle_send(xsend.at[pl.ds(1, pairs - 1), pl.ds(0, far)], rx_send.at[0])
    settle_send(xr.at[pl.ds(0, pairs)], sib_send.at[0])
    settle_send(part.at[pl.ds(0, pairs)], s1_send.at[0])
    settle_send(xr.at[0, pl.ds(0, far)], ret_send.at[0])
    settle_send(xr.at[pl.ds(0, pairs), pl.ds(1, far - 1)], ret_send.at[1])
    for name in ("out_rope", "out_latent", "out_result"):
        arrive(name)


def hand_over(result, latent, rope, out_result, out_latent, out_rope):
    out_result[...] = result[...]
    out_latent[...] = latent[...]
    out_rope[...] = rope[...]


def body(
    tokens,
    cache_latent,
    cache_rope,
    lengths,
    attn_gain,
    latent_gain,
    post_attn_gain,
    ffn_gain,
    post_ffn_gain,
    w_query,
    w_query_rot,
    w_latent,
    w_key_rot,
    w_key_up,
    w_value_up,
    w_out,
    route_logits,
    routes,
    w_gate,
    w_up,
    w_down,
):
    R, D = tokens.shape
    T = lax.axis_size("tp")
    EP = lax.axis_size("ep")
    C, LH, KD = w_key_up.shape
    RD = w_key_rot.shape[1]
    VD = w_value_up.shape[2]
    H = T * LH
    K = routes.shape[1]
    scale = (KD + RD) ** (-0.5)
    RP = 2 * SUB
    assert R == SUB + SUB // 2 and T % 2 == 0 and LH % 2 == 0
    assert EP & (EP - 1) == 0 and T * R <= LANES
    cap = (R * T * K + EP - 1) // EP + 1
    Q = D // T
    F = w_gate.shape[2]
    LC = w_latent.shape[1]
    SPAN = cache_latent.shape[1]
    N = T * R
    QL = Q // LANES
    FT, REST = cap // SUB, cap % SUB
    if REST > 1 or QL > SUB:
        FT, REST = -(-cap // SUB), 0
    W = FT * Q + REST * LANES
    far = EP // 2
    chunks = ((0, far), (far, far))
    table, places = layout(T, R, LH, chunks, FT, REST, QL)

    vm = pl.BlockSpec(memory_space=pltpu.VMEM)
    hbm = pl.BlockSpec(memory_space=pl.ANY)
    dma = pltpu.SemaphoreType.DMA
    pairs = T // 2
    ROT = LH * RD
    QW = (LH + LH // 2) * C + ROT + LC + ROT // 2 + LC

    def v(*shape, dtype=BF16):
        return pltpu.VMEM(shape, dtype)

    cfg = (T, EP, R, LH, FT, REST, chunks, scale, places)
    outs = pl.pallas_call(
        functools.partial(kernel, cfg),
        out_shape=(
            jax.ShapeDtypeStruct((R, D), BF16),
            jax.ShapeDtypeStruct((R, C), BF16),
            jax.ShapeDtypeStruct((R, RD), BF16),
        ),
        in_specs=[hbm] * 22,
        out_specs=(hbm, hbm, hbm),
        scratch_shapes=[
            pltpu.SMEM((R,), jnp.int32),
            v(R, D),
            v(D),
            v(C),
            v(D),
            v(D),
            v(D),
            v(K, N, dtype=jnp.int32),
            v(K, N, dtype=F32),
            v(R, D),
            v(R, C),
            v(R, RD),
            v(*table.shape),
            v(R, SPAN, C),
            v(R, RD, SPAN),
            v(D, LH * KD + ROT + LC),
            v(RD, D),
            v(C, LH * KD),
            v(C, LH * VD),
            v(LH * VD, D),
            v(D, 2 * F),
            v(F, D),
            v(T, SUB, D + D // 2),
            v(N, D),
            v(SUB, D, dtype=F32),
            v(T, SUB, QW),
            v(T, SUB, QW),
            v(R, H, C),
            v(R, H, RD),
            v(RP, C, dtype=F32),
            v(RP, RD, dtype=F32),
            v(R, H, C),
            v(T, SUB * LH, C),
            v(T, SUB * LH, C),
            v(T, (R - SUB) * LH, C),
            v(T, (R - SUB) * LH, C),
            v(T, N, Q),
            v(T, N, Q),
            v(T, N, Q),
            v(T, SUB, LANES, dtype=F32),
            v(T, RP, Q),
            v(T, RP, Q),
            v(pairs, EP, SUB, W),
            v(T, EP, SUB, W),
            v(T, EP, SUB, W),
            v(T, EP, SUB, W),
            v(pairs, EP, SUB, W),
            v(pairs, EP, SUB, W),
            v(pairs, EP, SUB, W),
            v(pairs, EP, SUB, W),
            v(T, RP, Q),
            v(T, RP, Q),
            v(T, pairs, RP, Q),
            v(T, pairs, RP, Q),
            v(len(chunks), T, QL * SUB, LANES, dtype=F32),
            v(len(chunks), T, far * SUB, LANES, dtype=F32),
            v(C, LH, KD),
            v(C, LH, VD),
            v(C * LH, KD, dtype=F32),
            v(R, H, SPAN, dtype=F32),
            v(R, H, SPAN),
            dma((19,)),
            dma((3,)),
            dma((10,)),
            dma((1,)),
            dma((pairs,)),
            dma((2,)),
            dma((EP,)),
            dma((1,)),
            dma((far, max(1, pairs - 1))),
            dma((1,)),
            dma((len(chunks),)),
            dma((1,)),
            dma((len(chunks), pairs)),
            dma((1,)),
            dma((far, max(1, pairs - 1))),
            dma((2,)),
            dma((2,)),
            pltpu.SemaphoreType.REGULAR((max(1, EP.bit_length() - 2),)),
        ],
        compiler_params=pltpu.CompilerParams(
            collective_id=0, has_side_effects=True, vmem_limit_bytes=60 * 1024 * 1024
        ),
    )(
        lengths,
        tokens,
        attn_gain,
        latent_gain,
        post_attn_gain,
        ffn_gain,
        post_ffn_gain,
        routes.T,
        route_logits.T,
        jnp.asarray(table, BF16),
        cache_latent,
        cache_rope,
        w_query,
        w_query_rot,
        w_latent,
        w_key_rot.T,
        w_key_up,
        w_value_up,
        w_out,
        w_gate,
        w_up,
        w_down,
    )
    return pl.pallas_call(
        hand_over,
        out_shape=tuple(jax.ShapeDtypeStruct(o.shape, o.dtype) for o in outs),
        in_specs=[vm] * 3,
        out_specs=(vm, vm, vm),
    )(*outs)


def solution(mesh):
    return jax.shard_map(
        body,
        mesh=mesh,
        in_specs=(
            P(("ep", "tp"), None),
            P(("ep", "tp"), None, None),
            P(("ep", "tp"), None, None),
            P(("ep", "tp")),
            P(),
            P(),
            P(),
            P(),
            P(),
            P(None, "tp"),
            P(None, "tp"),
            P(None, "tp"),
            P(),
            P(None, "tp", None),
            P(None, "tp", None),
            P("tp", None),
            P("ep", None),
            P("ep", None),
            P("ep", None, "tp"),
            P("ep", None, "tp"),
            P("ep", "tp", None),
        ),
        out_specs=(P(("ep", "tp"), None), P(("ep", "tp"), None), P(("ep", "tp"), None)),
        check_vma=False,
    )
```
